256 devices in a mesh: dp: 4 (over x), kv: 32 (over z, y), tp: 2 (over core).
Axes of the slice: x: 4, y: 4, z: 8, core: 2. Of those that a mesh axis runs over, the one named last changes fastest.
Arguments:
- hidden_in: bfloat16 [384, 2048], P('dp', ('kv', 'tp')), may hold values from -21 to 21
- state: float32 [384, 16, 128, 128], P(('dp', 'kv'), 'tp'), may hold values from -6 to 6
- forget_floor: float32 [16, 128], P('tp'), may hold values from 0 to 0.9
- ffn_gain_one: float32 [2048], replicated, may hold values from 0.1 to 1.9
- w_gate_one: bfloat16 [2048, 5632], P(None, ('kv', 'tp')), may hold values from -0.125 to 0.125
- w_up_one: bfloat16 [2048, 5632], P(None, ('kv', 'tp')), may hold values from -0.125 to 0.125
- w_down_one: bfloat16 [5632, 2048], P(('kv', 'tp')), may hold values from -0.21875 to 0.21875
- mix_gain: float32 [2048], replicated, may hold values from 0.1 to 1.9
- w_query: bfloat16 [2048, 16, 128], P(None, 'tp', 'kv'), may hold values from -0.125 to 0.125
- w_forget: bfloat16 [2048, 16, 128], P(None, 'tp', 'kv'), may hold values from -0.125 to 0.125
- w_input: bfloat16 [2048, 16, 128], P(None, 'tp', 'kv'), may hold values from -0.125 to 0.125
- w_outgate: bfloat16 [2048, 16, 128], P(None, 'tp', 'kv'), may hold values from -0.125 to 0.125
- head_gain: float32 [16, 128], P('tp'), may hold values from 0.1 to 1.9
- w_mix_out: bfloat16 [2048, 2048], P(None, ('kv', 'tp')), may hold values from -0.125 to 0.125
- ffn_gain_two: float32 [2048], replicated, may hold values from 0.1 to 1.9
- w_gate_two: bfloat16 [2048, 5632], P(None, ('kv', 'tp')), may hold values from -0.125 to 0.125
- w_up_two: bfloat16 [2048, 5632], P(None, ('kv', 'tp')), may hold values from -0.125 to 0.125
- w_down_two: bfloat16 [5632, 2048], P(('kv', 'tp')), may hold values from -0.21875 to 0.21875
Outputs:
- output_rows: bfloat16 [384, 2048], P('dp', ('kv', 'tp'))
- new_state: float32 [384, 16, 128, 128], P(('dp', 'kv'), 'tp')
The draws below stay inside these ranges and needn't reach their ends.
All inputs are finite; a program needn't handle non-finite values.
Results may differ from the reference program's by a relative error of at most 0.009.
Values may be sent and summed in bfloat16 or wider, within the bound.
No kernel may reach another device: no remote copies, remote signals or barrier semaphores. Data moves between devices by JAX's collectives and lax.ppermute only.
A program may use at most 64 MiB of HBM per device.

```python
import jax
import jax.numpy as jnp
from jax import lax

WIDTH = 2048
HEADS = 16
KEY_DIM = 128
VALUE_DIM = 128
FFN_DIM = 5632
SEQS = 384


def draw_hidden_in(key, part):
    base_key = jax.random.fold_in(key, 11)
    scale_key, value_key = jax.random.split(base_key, 2)
    position = jnp.arange(WIDTH, dtype=jnp.float32) / WIDTH
    jitter = jax.random.uniform(scale_key, (WIDTH,), jnp.float32, -0.3, 0.3)
    column_scale = 0.5 * jnp.exp(jnp.log(10.0) * position + jitter)
    values = jnp.clip(jax.random.normal(value_key, (SEQS, WIDTH), jnp.float32), -3.0, 3.0)
    return (values * column_scale[None, :]).astype(jnp.bfloat16)


def raised(entries, own_key, source, target, blocks, factor):
    owner, partner = [(jnp.arange(entries.shape[axis_at]) // (entries.shape[axis_at] // blocks)).reshape([-1 if axis == axis_at else 1 for axis in range(entries.ndim)]) for axis_at in (source, target)]
    chosen = jax.random.permutation(own_key, blocks)[partner]
    strong = (owner == chosen) | (owner == (partner + blocks // 2) % blocks)
    return jnp.where(strong, factor * entries, entries)


def block_levels(rng, extent, cuts, smallest, high):
    gain = 1.0
    for axis_at, shards_of in cuts:
        heights = jax.random.uniform(jax.random.fold_in(jax.random.fold_in(rng, 6), axis_at), (shards_of,), jnp.float32, smallest / len(cuts), high / len(cuts))
        gain = gain * jnp.repeat(jnp.exp(heights), extent[axis_at] // shards_of).reshape((-1,) + (1,) * (len(extent) - 1 - axis_at))
    return gain


def scatter_about(rng, dims, scale, reach, cuts=(), held_as=jnp.bfloat16):
    loudness = block_levels(rng, dims, cuts, -0.22, 0.18) if cuts else 1.0
    values = jax.random.normal(rng, dims, jnp.float32) * scale * loudness
    return jnp.minimum(jnp.maximum(values, -reach), reach).astype(held_as)


def gaussian_with(stream_key, shape, width, bound, pieces, heavy, kind=jnp.bfloat16):
    entries = width * jax.random.normal(stream_key, shape, jnp.float32)
    if pieces:
        entries = entries * block_levels(stream_key, shape, pieces, -0.22, 0.18)
    return jnp.clip(raised(entries, jax.random.fold_in(stream_key, 3), *heavy), -bound, bound).astype(kind)


def setup_inputs(seed: int = 0) -> dict:
    splits = jax.random.split(jax.random.key(seed), 19)
    hidden_in = draw_hidden_in(jax.random.fold_in(splits[18], 71), 0)
    state = scatter_about(splits[1], (SEQS, HEADS, KEY_DIM, VALUE_DIM), 1.0, 6.0, ((0, 128), (1, 2)), jnp.float32)
    forget_floor = jnp.clip(0.9 * jax.random.uniform(splits[2], (HEADS, KEY_DIM), jnp.float32) ** block_levels(splits[2], (HEADS, KEY_DIM), ((0, 2),), -0.2, 0.2), 0.0, 0.9)
    ffn_gain_one = jnp.clip(1.0 + 0.18 * jax.random.normal(splits[3], (WIDTH,), jnp.float32), 0.1, 1.9)
    w_gate_one = scatter_about(splits[4], (WIDTH, FFN_DIM), WIDTH ** -0.5, 0.125, ((1, 64),))
    w_up_one = scatter_about(splits[5], (WIDTH, FFN_DIM), WIDTH ** -0.5, 0.125, ((1, 64),))
    w_down_one = gaussian_with(splits[6], (FFN_DIM, WIDTH), FFN_DIM ** -0.5, 0.21875, ((0, 64),), (0, 1, 64, 4.0))
    mix_gain = jnp.clip(1.0 + 0.18 * jax.random.normal(splits[7], (WIDTH,), jnp.float32), 0.1, 1.9)
    w_query = scatter_about(splits[8], (WIDTH, HEADS, KEY_DIM), WIDTH ** -0.5, 0.125, ((1, 2), (2, 32)))
    w_forget = scatter_about(splits[9], (WIDTH, HEADS, KEY_DIM), WIDTH ** -0.5, 0.125, ((1, 2), (2, 32)))
    w_input = scatter_about(splits[10], (WIDTH, HEADS, VALUE_DIM), WIDTH ** -0.5, 0.125, ((1, 2), (2, 32)))
    w_outgate = scatter_about(splits[11], (WIDTH, HEADS, VALUE_DIM), WIDTH ** -0.5, 0.125, ((1, 2), (2, 32)))
    head_gain = jnp.clip(1.0 + 0.18 * jax.random.normal(splits[12], (HEADS, VALUE_DIM), jnp.float32), 0.1, 1.9)
    w_mix_out = scatter_about(splits[13], (WIDTH, WIDTH), WIDTH ** -0.5, 0.125, ((1, 64),))
    ffn_gain_two = jnp.clip(1.0 + 0.18 * jax.random.normal(splits[14], (WIDTH,), jnp.float32), 0.1, 1.9)
    w_gate_two = scatter_about(splits[15], (WIDTH, FFN_DIM), WIDTH ** -0.5, 0.125, ((1, 64),))
    w_up_two = scatter_about(splits[16], (WIDTH, FFN_DIM), WIDTH ** -0.5, 0.125, ((1, 64),))
    w_down_two = gaussian_with(splits[17], (FFN_DIM, WIDTH), FFN_DIM ** -0.5, 0.21875, ((0, 64),), (0, 1, 64, 4.0))
    return {"hidden_in": hidden_in, "state": state, "forget_floor": forget_floor, "ffn_gain_one": ffn_gain_one, "w_gate_one": w_gate_one, "w_up_one": w_up_one, "w_down_one": w_down_one, "mix_gain": mix_gain, "w_query": w_query, "w_forget": w_forget, "w_input": w_input, "w_outgate": w_outgate, "head_gain": head_gain, "w_mix_out": w_mix_out, "ffn_gain_two": ffn_gain_two, "w_gate_two": w_gate_two, "w_up_two": w_up_two, "w_down_two": w_down_two}


EPS = 1e-06

def normed_rows(rows_in, gain_vec):
    values = rows_in.astype(jnp.float32)
    row_scale = lax.rsqrt(lax.optimization_barrier(jnp.mean(values * values, axis=1, keepdims=True)) + EPS)
    return (values * row_scale * gain_vec[None, :]).astype(jnp.bfloat16)

def half_mlp(rows_in, gain_vec, w_gate, w_upper, w_lower):
    normed = normed_rows(rows_in, gain_vec)
    gate_act = jnp.dot(normed, w_gate, preferred_element_type=jnp.float32)
    upper = jnp.dot(normed, w_upper, preferred_element_type=jnp.float32)
    hidden_mid = (jax.nn.silu(gate_act) * upper).astype(jnp.bfloat16)
    lowered = jnp.dot(hidden_mid, w_lower, preferred_element_type=jnp.float32)
    return (rows_in.astype(jnp.float32) + 0.5 * lowered).astype(jnp.bfloat16)

def project(normed, weight):
    flat = jnp.dot(normed, weight.reshape(weight.shape[0], -1), preferred_element_type=jnp.float32)
    return flat.astype(jnp.bfloat16).reshape(normed.shape[0], weight.shape[1], weight.shape[2])

def reference(hidden_in, state, forget_floor, ffn_gain_one, w_gate_one, w_up_one, w_down_one, mix_gain, w_query, w_forget, w_input, w_outgate, head_gain, w_mix_out, ffn_gain_two, w_gate_two, w_up_two, w_down_two):
    after_one = half_mlp(hidden_in, ffn_gain_one, w_gate_one, w_up_one, w_down_one)
    normed_mix = normed_rows(after_one, mix_gain)
    query = project(normed_mix, w_query).astype(jnp.float32)
    forget_pre = project(normed_mix, w_forget).astype(jnp.float32)
    inputs = project(normed_mix, w_input).astype(jnp.float32)
    out_gate = project(normed_mix, w_outgate).astype(jnp.float32)
    forget = forget_floor[None] + (1.0 - forget_floor[None]) * jax.nn.sigmoid(forget_pre)
    keep_in = (1.0 - forget_floor[None]) * jax.nn.sigmoid(-forget_pre)
    new_state = forget[..., None] * state + keep_in[..., None] * inputs[:, :, None, :]
    readout = jnp.einsum('shk,shkv->shv', query, new_state, precision=lax.Precision.HIGHEST)
    head_scale = lax.rsqrt(lax.optimization_barrier(jnp.mean(readout * readout, axis=2, keepdims=True)) + EPS)
    gated = readout * head_scale * head_gain[None] * jax.nn.silu(out_gate)
    merged = gated.reshape(hidden_in.shape[0], WIDTH).astype(jnp.bfloat16)
    mixed = jnp.dot(merged, w_mix_out, preferred_element_type=jnp.float32)
    after_mix = (after_one.astype(jnp.float32) + mixed).astype(jnp.bfloat16)
    output_rows = half_mlp(after_mix, ffn_gain_two, w_gate_two, w_up_two, w_down_two)
    return (output_rows, new_state)
```

```python
import jax
import jax.numpy as jnp
from jax import lax
from jax.sharding import PartitionSpec as P

EPS = 1e-06


def copy_for_each(x, axis):
    copies = jnp.broadcast_to(x, (lax.axis_size(axis), *x.shape))
    return lax.all_to_all(copies, axis, split_axis=0, concat_axis=0, tiled=True)


def swap_cores(x):
    return lax.ppermute(x, "tp", [(0, 1), (1, 0)])


def pair_of_cores(own, other, dim):
    first = lax.axis_index("tp") == 0
    return jnp.stack([jnp.where(first, own, other), jnp.where(first, other, own)], axis=dim)


def gathered_columns(x):
    own = copy_for_each(x, "kv")
    tiles = pair_of_cores(own, swap_cores(own), 1)
    return jnp.moveaxis(tiles, 2, 0).reshape(x.shape[0], -1)


def sent_and_summed(partial):
    rows = partial.shape[0]
    kv_count, tp_count = (lax.axis_size("kv"), lax.axis_size("tp"))
    blocks = partial.reshape(rows, kv_count, tp_count, -1)
    first = lax.axis_index("tp") == 0
    own = jnp.where(first, blocks[:, :, 0], blocks[:, :, 1])
    other = jnp.where(first, blocks[:, :, 1], blocks[:, :, 0])
    from_other = swap_cores(other.astype(jnp.bfloat16))
    both = (own + from_other.astype(jnp.float32)).astype(jnp.bfloat16)
    tiles = jnp.moveaxis(both, 1, 0)
    arrived = lax.all_to_all(tiles, "kv", split_axis=0, concat_axis=0, tiled=True)
    return arrived.astype(jnp.float32).sum(axis=0)


def sent_together(arrays, axis, split_dim, concat_dim, along):
    widths = [a.shape[along] for a in arrays]
    both = jnp.concatenate(arrays, axis=along)
    whole = lax.all_to_all(both, axis, split_axis=split_dim, concat_axis=concat_dim, tiled=True)
    return tuple(jnp.split(whole, [sum(widths[:k]) for k in range(1, len(widths))], axis=along))


def local_norm(full_rows, gain_vec):
    values = full_rows.astype(jnp.float32)
    row_scale = lax.rsqrt(jnp.mean(values * values, axis=1, keepdims=True) + EPS)
    return (values * row_scale * gain_vec[None, :]).astype(jnp.bfloat16)


def spread_norm(shard_in, gain_vec):
    full_rows = gathered_columns(shard_in)
    return local_norm(full_rows, gain_vec)


def mlp_term(normed, w_gate, w_upper, w_lower):
    gate_act = jnp.dot(normed, w_gate, preferred_element_type=jnp.float32)
    upper = jnp.dot(normed, w_upper, preferred_element_type=jnp.float32)
    hidden_mid = (jax.nn.silu(gate_act) * upper).astype(jnp.bfloat16)
    return jnp.dot(hidden_mid, w_lower, preferred_element_type=jnp.float32)


def project(normed, weight):
    flat = jnp.einsum("rd,dhk->rhk", normed, weight, preferred_element_type=jnp.float32)
    return flat.astype(jnp.bfloat16)


def shards(
    hidden_in,
    state,
    forget_floor,
    ffn_gain_one,
    w_gate_one,
    w_up_one,
    w_down_one,
    mix_gain,
    w_query,
    w_forget,
    w_input,
    w_outgate,
    head_gain,
    w_mix_out,
    ffn_gain_two,
    w_gate_two,
    w_up_two,
    w_down_two,
):
    columns = hidden_in.shape[1]
    normed_one = spread_norm(hidden_in, ffn_gain_one)
    ffn_term = mlp_term(normed_one, w_gate_one, w_up_one, w_down_one)
    summed_one = sent_and_summed(ffn_term)
    after_own = (hidden_in.astype(jnp.float32) + 0.5 * summed_one).astype(jnp.bfloat16)
    after_rows = gathered_columns(after_own)
    normed_mix = local_norm(after_rows, mix_gain)
    projected = (
        project(normed_mix, w_query),
        project(normed_mix, w_forget),
        project(normed_mix, w_input),
        project(normed_mix, w_outgate),
    )
    query, forget_pre, inputs, out_gate = sent_together(
        (projected[0], projected[1], projected[2], projected[3]), "kv", 0, 2, 1
    )
    forget_raw = forget_pre.astype(jnp.float32)
    forget = forget_floor[None] + (1.0 - forget_floor[None]) * jax.nn.sigmoid(forget_raw)
    keep_in = (1.0 - forget_floor[None]) * jax.nn.sigmoid(-forget_raw)
    new_state = (
        forget[..., None] * state + keep_in[..., None] * inputs.astype(jnp.float32)[:, :, None, :]
    )
    readout = jnp.einsum(
        "shk,shkv->shv", query.astype(jnp.float32), new_state, precision=lax.Precision.HIGHEST
    )
    head_scale = lax.rsqrt(jnp.mean(readout * readout, axis=2, keepdims=True) + EPS)
    gated = readout * head_scale * head_gain[None] * jax.nn.silu(out_gate.astype(jnp.float32))
    seq_count = gated.shape[0]
    merged = gated.reshape(seq_count, -1).astype(jnp.bfloat16)
    own_heads = copy_for_each(merged, "kv").reshape(-1, merged.shape[1])
    heads = pair_of_cores(own_heads, swap_cores(own_heads), 1)
    weight_blocks = w_mix_out.reshape(lax.axis_size("tp"), merged.shape[1], columns)
    mixed = jnp.einsum("rtc,tcd->rd", heads, weight_blocks, preferred_element_type=jnp.float32)
    after_mix = (after_own.astype(jnp.float32) + mixed).astype(jnp.bfloat16)
    normed_two = spread_norm(after_mix, ffn_gain_two)
    summed_two = sent_and_summed(mlp_term(normed_two, w_gate_two, w_up_two, w_down_two))
    output_rows = (after_mix.astype(jnp.float32) + 0.5 * summed_two).astype(jnp.bfloat16)
    return (output_rows, new_state)


def solution(mesh):
    return jax.shard_map(
        shards,
        mesh=mesh,
        in_specs=(
            P("dp", ("kv", "tp")),
            P(("dp", "kv"), "tp", None, None),
            P("tp", None),
            P(),
            P(None, ("kv", "tp")),
            P(None, ("kv", "tp")),
            P(("kv", "tp"), None),
            P(),
            P(None, "tp", "kv"),
            P(None, "tp", "kv"),
            P(None, "tp", "kv"),
            P(None, "tp", "kv"),
            P("tp", None),
            P(None, ("kv", "tp")),
            P(),
            P(None, ("kv", "tp")),
            P(None, ("kv", "tp")),
            P(("kv", "tp"), None),
        ),
        out_specs=(P("dp", ("kv", "tp")), P(("dp", "kv"), "tp", None, None)),
        check_vma=False,
    )
```

```python
import jax
import jax.numpy as jnp
from jax import lax
from jax.sharding import PartitionSpec as P

EPS = 1e-06
LANES = 128


def groups_of(mesh):
    z_count, y_count = PLANE
    tp_count = mesh.shape["tp"]
    return [
        [(z * y_count + y) * tp_count + t for z in range(z_count) for t in range(tp_count)]
        for y in range(y_count)
    ]


PLANE = (8, 4)


def bf(x):
    return x.astype(jnp.bfloat16)


def f32(x):
    return x.astype(jnp.float32)


def matmul(a, b, dims):
    return lax.dot_general(a, b, (dims, ((), ())), preferred_element_type=jnp.float32)


def exchange(tiles, axis, groups=None):
    return lax.all_to_all(
        tiles, axis, split_axis=0, concat_axis=0, axis_index_groups=groups, tiled=True
    )


def copies(x, count):
    return jnp.broadcast_to(x, (count, *x.shape))


def swap_cores(x):
    return lax.ppermute(x, "tp", [(0, 1), (1, 0)])


def shift_y(x, step):
    z_count, y_count = PLANE
    pairs = [
        (z * y_count + y, z * y_count + (y + step) % y_count)
        for z in range(z_count)
        for y in range(y_count)
    ]
    return lax.ppermute(x, "kv", pairs)


def one_hot(targets, count, axis):
    shape = [targets.shape[0], targets.shape[0]]
    shape[axis] = count
    ids = lax.broadcasted_iota(jnp.int32, tuple(shape), axis)
    return (ids == jnp.expand_dims(targets, axis)).astype(jnp.bfloat16)


def norm_rows(rows, gain):
    values = f32(rows)
    scale = lax.rsqrt(jnp.mean(values * values, axis=1, keepdims=True) + EPS)
    return bf(values * scale * gain[None, :])


def by_y(parts, y, axis):
    count = len(parts)
    stacked = jnp.stack(parts, axis=0)
    ordered = [
        lax.dynamic_index_in_dim(stacked, (y - k + count) % count, 0, keepdims=False)
        for k in range(count)
    ]
    return jnp.stack(ordered, axis=axis)


def split_cores(blocks, first):
    own = jnp.where(first, blocks[..., 0, :], blocks[..., 1, :])
    other = jnp.where(first, blocks[..., 1, :], blocks[..., 0, :])
    return own, other


def make_shards(slab_groups):
    z_count, y_count = PLANE

    def shards(
        hidden_in,
        state,
        forget_floor,
        ffn_gain_one,
        w_gate_one,
        w_up_one,
        w_down_one,
        mix_gain,
        w_query,
        w_forget,
        w_input,
        w_outgate,
        head_gain,
        w_mix_out,
        ffn_gain_two,
        w_gate_two,
        w_up_two,
        w_down_two,
    ):
        rows, own_cols = hidden_in.shape
        width = w_gate_one.shape[0]
        seqs, heads, key_dim, _ = state.shape
        kv_count, tp_count = z_count * y_count, lax.axis_size("tp")
        slab_rows = rows // y_count
        hidden_two = w_gate_two.shape[1]
        kv = lax.axis_index("kv")
        z, y = kv // y_count, kv % y_count
        core = lax.axis_index("tp")
        first = core == 0

        def slab_exchange(x):
            return exchange(copies(x, z_count * tp_count), ("kv", "tp"), slab_groups)

        proj_w = jnp.concatenate(
            [jnp.transpose(w, (1, 2, 0)) for w in (w_query, w_forget, w_input, w_outgate)], axis=0
        )
        late_w = jnp.concatenate(
            [w_mix_out.T, w_gate_two.T, w_up_two.T, w_down_two], axis=0
        )

        def along_y(w):
            below, above = shift_y(w, 1), shift_y(w, -1)
            return [w, below, shift_y(below, 1), above]

        proj_parts = along_y(proj_w)
        late_parts = along_y(late_w)

        new_rows = jnp.arange(rows, dtype=jnp.int32)
        old_rows = (
            (new_rows % slab_rows) // seqs * (y_count * seqs)
            + new_rows // slab_rows * seqs
            + new_rows % seqs
        )
        reorder = one_hot(old_rows, rows, 1)
        hidden_own = bf(matmul(reorder, hidden_in, ((1,), (0,))))
        own = exchange(copies(hidden_own, kv_count), "kv")
        other = swap_cores(own)
        tiles = jnp.stack(
            [jnp.where(first, own, other), jnp.where(first, other, own)], axis=1
        )
        hidden_rows = jnp.moveaxis(tiles, 2, 0).reshape(rows, width)
        normed = norm_rows(hidden_rows, ffn_gain_one)
        gate = matmul(normed, w_gate_one, ((1,), (0,)))
        upper = matmul(normed, w_up_one, ((1,), (0,)))
        mid = bf(jax.nn.silu(gate) * upper)
        lowered = matmul(mid, w_down_one, ((1,), (0,)))
        lowered = lowered.reshape(rows, z_count, tp_count, LANES)
        mine, theirs = split_cores(lowered, first)
        both = bf(mine + f32(swap_cores(bf(theirs))))
        tiles = both.reshape(y_count, slab_rows, z_count, LANES)
        tiles = jnp.transpose(tiles, (2, 0, 1, 3)).reshape(kv_count, slab_rows, LANES)
        summed = f32(exchange(tiles, "kv")).sum(axis=0)
        hidden_slab = lax.dynamic_slice(
            hidden_rows,
            (y * slab_rows, (z * tp_count + core) * LANES),
            (slab_rows, LANES),
        )
        after_own = bf(f32(hidden_slab) + 0.5 * summed)

        after_rows = jnp.moveaxis(slab_exchange(after_own), 0, 1).reshape(slab_rows, width)
        normed = norm_rows(after_rows, mix_gain)
        projected = [
            bf(matmul(normed, w.reshape(-1, width), ((1,), (1,)))) for w in proj_parts
        ]
        channels = by_y(projected, y, 1)
        channels = channels.reshape(z_count, seqs * y_count, LANES)
        zgroups = [[a * y_count + b for a in range(z_count)] for b in range(y_count)]
        arrived = exchange(channels, "kv", zgroups)
        arrived = arrived.reshape(z_count, seqs, y_count, LANES)
        arrived = jnp.moveaxis(arrived, 1, 0).reshape(seqs, kv_count, LANES)
        per = w_query.shape[2]
        lanes = jnp.arange(LANES, dtype=jnp.int32)
        spread = one_hot(lanes // per, kv_count, 1)
        keep = (lanes[:, None] % per == lanes[None, :] % per).astype(jnp.bfloat16)
        gather = one_hot(lanes // per, LANES // per, 1)
        spreads = jnp.broadcast_to(spread, (seqs, *spread.shape))
        wide = lax.dot_general(
            spreads, arrived, (((2,), (1,)), ((0,), (0,))), preferred_element_type=jnp.float32
        )
        wide = bf(wide) * keep[None]
        gathers = jnp.broadcast_to(gather, (seqs, *gather.shape))
        kinds = lax.dot_general(
            gathers, wide, (((1,), (2,)), ((0,), (0,))), preferred_element_type=jnp.float32
        )
        kinds = kinds.reshape(seqs, 4, heads, key_dim)
        query, forget_raw, inputs, out_gate = (kinds[:, k] for k in range(4))
        forget = forget_floor[None] + (1.0 - forget_floor[None]) * jax.nn.sigmoid(forget_raw)
        keep_in = (1.0 - forget_floor[None]) * jax.nn.sigmoid(-forget_raw)
        new_state = forget[..., None] * state + keep_in[..., None] * inputs[:, :, None, :]
        readout = jnp.einsum(
            "shk,shkv->shv", query, new_state, precision=lax.Precision.HIGHEST
        )
        head_scale = lax.rsqrt(jnp.mean(readout * readout, axis=2, keepdims=True) + EPS)
        gated = readout * head_scale * head_gain[None] * jax.nn.silu(out_gate)
        merged = bf(gated.reshape(seqs, -1))

        merged_rows = slab_exchange(merged).reshape(z_count, tp_count, seqs, merged.shape[1])
        merged_rows = jnp.transpose(merged_rows, (0, 2, 1, 3)).reshape(slab_rows, width)
        mixed = [matmul(merged_rows, w[:own_cols], ((1,), (1,))) for w in late_parts]
        mixed = by_y(mixed, y, 1)
        residual = lax.dynamic_slice(
            after_rows, (0, z * y_count * tp_count * own_cols), (slab_rows, 2 * LANES)
        ).reshape(slab_rows, y_count, tp_count, own_cols)
        residual = jnp.where(first, residual[:, :, 0], residual[:, :, 1])
        after_mix = bf(f32(residual) + mixed).reshape(slab_rows, LANES)

        tiles = slab_exchange(after_mix).reshape(z_count, tp_count, slab_rows, LANES)
        tiles = jnp.transpose(tiles, (0, 2, 1, 3)).reshape(z_count * slab_rows, 2 * LANES)
        wide_lanes = jnp.arange(2 * LANES, dtype=jnp.int32)
        natural = (
            wide_lanes % LANES // own_cols * (tp_count * own_cols)
            + wide_lanes // LANES * own_cols
            + wide_lanes % own_cols
        )
        to_natural = one_hot(natural, 2 * LANES, 1)
        ordered = bf(matmul(tiles, to_natural, ((1,), (0,))))
        mix_rows = jnp.moveaxis(ordered.reshape(z_count, slab_rows, 2 * LANES), 0, 1)
        normed = norm_rows(mix_rows.reshape(slab_rows, width), ffn_gain_two)
        low, high = own_cols, own_cols + hidden_two
        total = None
        for w in late_parts:
            gate = matmul(normed, w[low:high], ((1,), (1,)))
            upper = matmul(normed, w[high : high + hidden_two], ((1,), (1,)))
            mid = bf(jax.nn.silu(gate) * upper)
            part = matmul(mid, w[high + hidden_two :], ((1,), (0,)))
            total = part if total is None else total + part
        total = bf(0.5 * total).reshape(slab_rows * z_count, 2 * LANES)
        split = matmul(total, to_natural, ((1,), (1,)))
        split = split.reshape(slab_rows, z_count, tp_count, LANES)
        mine, theirs = split_cores(split, first)
        both = mine + f32(swap_cores(bf(theirs)))
        at_home = lax.broadcasted_iota(jnp.int32, (1, z_count, 1), 1) == z
        both = bf(both + jnp.where(at_home, f32(after_mix)[:, None], 0.0))
        tiles = jnp.broadcast_to(
            jnp.moveaxis(both, 0, 1)[:, None], (z_count, y_count, slab_rows, LANES)
        ).reshape(kv_count, slab_rows, LANES)
        arrived = exchange(tiles, "kv").reshape(z_count, rows, LANES)
        result = bf(f32(arrived).sum(axis=0))
        pick = one_hot(y * own_cols + jnp.arange(own_cols, dtype=jnp.int32), LANES, 0)
        result = bf(matmul(result, pick, ((1,), (0,))))
        output_rows = bf(matmul(reorder, result, ((0,), (0,))))
        return (output_rows, new_state)

    return shards


def solution(mesh):
    return jax.shard_map(
        make_shards(groups_of(mesh)),
        mesh=mesh,
        in_specs=(
            P("dp", ("kv", "tp")),
            P(("dp", "kv"), "tp", None, None),
            P("tp", None),
            P(),
            P(None, ("kv", "tp")),
            P(None, ("kv", "tp")),
            P(("kv", "tp"), None),
            P(),
            P(None, "tp", "kv"),
            P(None, "tp", "kv"),
            P(None, "tp", "kv"),
            P(None, "tp", "kv"),
            P("tp", None),
            P(None, ("kv", "tp")),
            P(),
            P(None, ("kv", "tp")),
            P(None, ("kv", "tp")),
            P(("kv", "tp"), None),
        ),
        out_specs=(P("dp", ("kv", "tp")), P(("dp", "kv"), "tp", None, None)),
        check_vma=False,
    )
```

```python
import jax
import jax.numpy as jnp
from jax import lax
from jax.experimental import pallas as pl
from jax.experimental.pallas import tpu as pltpu
from jax.sharding import PartitionSpec as P

EPS = 1e-06
LANES = 128
Z_COUNT, Y_COUNT, TP_COUNT = 8, 4, 2
KV_COUNT = Z_COUNT * Y_COUNT
NN, NT = ((1,), (0,)), ((1,), (1,))


def bf(x):
    return x.astype(jnp.bfloat16)


def f32(x):
    return x.astype(jnp.float32)


def matmul(a, b, dims):
    return lax.dot_general(a, b, (dims, ((), ())), preferred_element_type=jnp.float32)


def exchange(tiles, axis, groups=None):
    return lax.all_to_all(
        tiles, axis, split_axis=0, concat_axis=0, axis_index_groups=groups, tiled=True
    )


def copies(x, count):
    return jnp.broadcast_to(x, (count, *x.shape))


def swap_cores(x):
    return lax.ppermute(x, "tp", [(0, 1), (1, 0)])


def shift_y(x, step):
    pairs = [
        (z * Y_COUNT + y, z * Y_COUNT + (y + step) % Y_COUNT)
        for z in range(Z_COUNT)
        for y in range(Y_COUNT)
    ]
    return lax.ppermute(x, "kv", pairs)


def slab_exchange(x):
    groups = [
        [(z * Y_COUNT + y) * TP_COUNT + t for z in range(Z_COUNT) for t in range(TP_COUNT)]
        for y in range(Y_COUNT)
    ]
    return exchange(copies(x, Z_COUNT * TP_COUNT), ("kv", "tp"), groups)


def place():
    kv = lax.axis_index("kv")
    return lax.div(kv, Y_COUNT), lax.rem(kv, Y_COUNT), lax.axis_index("tp")


def iota(shape, axis):
    return lax.broadcasted_iota(jnp.int32, shape, axis)


def hot(mask):
    return jnp.where(mask, 1.0, 0.0).astype(jnp.bfloat16)


def local(body, outs, *args, scratch=(), outside=(), vmem=False, flops=1 << 20):
    kind = pltpu.VMEM if vmem else jax.ShapeDtypeStruct
    shapes = [kind(s, d) for s, d in outs]
    held = pl.BlockSpec(memory_space=pltpu.VMEM)
    specs = [pl.BlockSpec(memory_space=pl.ANY) if k in outside else held for k in range(len(args))]
    args = [
        pltpu.with_memory_space_constraint(a, pltpu.HBM) if k in outside else a
        for k, a in enumerate(args)
    ]
    size = sum(a.size * a.dtype.itemsize for a in args)
    return pl.pallas_call(
        body,
        out_shape=shapes,
        in_specs=specs,
        out_specs=[held] * len(outs),
        scratch_shapes=list(scratch),
        compiler_params=pltpu.CompilerParams(vmem_limit_bytes=VMEM_LIMIT),
        cost_estimate=pl.CostEstimate(flops=flops, bytes_accessed=size, transcendentals=0),
    )(*args)


VMEM_LIMIT = 24 * 1024 * 1024


def first_block(
    own, other, gain, w_gate, w_up, w_down, mine, theirs, slab, xt, low, gate_w, up_w, down_w, sems
):
    z, y, core = place()
    moves = [
        pltpu.make_async_copy(src, dst, sems.at[k])
        for k, (src, dst) in enumerate(((w_gate, gate_w), (w_up, up_w), (w_down, down_w)))
    ]
    for move in moves:
        move.start()
    cols = own.shape[1]
    for kv in range(KV_COUNT):
        base = kv * TP_COUNT * cols
        xt[pl.ds(pl.multiple_of(base + core * cols, cols), cols), :] = own[kv]
        xt[pl.ds(pl.multiple_of(base + (1 - core) * cols, cols), cols), :] = other[kv]
    width, rows = xt.shape
    square = jnp.zeros((8, rows), jnp.float32)
    for c in range(width // LANES):
        part = f32(xt[c * LANES : (c + 1) * LANES, :])
        square += (part * part).reshape(LANES // 8, 8, rows).sum(axis=0)
    scale = lax.rsqrt(square.sum(axis=0, keepdims=True) * (1.0 / width) + EPS)
    gains = gain[...].T
    normed = []
    for c in range(width // LANES):
        part = f32(xt[c * LANES : (c + 1) * LANES, :])
        normed.append(bf(part * scale * gains[:, c : c + 1]))
    normed = jnp.concatenate(normed, axis=0)
    moves[0].wait()
    gate = matmul(gate_w[...], normed, NN)
    moves[1].wait()
    upper = matmul(up_w[...], normed, NN)
    mid = bf(jax.nn.silu(gate) * upper)
    count = slab.shape[0]
    seqs = count // Z_COUNT
    new, old = iota((rows, rows), 0), iota((rows, rows), 1)
    wanted = (
        lax.div(lax.rem(new, count), seqs) * (Y_COUNT * seqs)
        + lax.div(new, count) * seqs
        + lax.rem(new, seqs)
    )
    mid = bf(matmul(hot(old == wanted), mid, NT))
    moves[2].wait()
    low[...] = matmul(mid, down_w[...], NN)
    for k in range(Z_COUNT):
        at = pl.multiple_of((k * TP_COUNT + core) * LANES, LANES)
        to = pl.multiple_of((k * TP_COUNT + 1 - core) * LANES, LANES)
        mine[k] = low[:, pl.ds(at, LANES)]
        theirs[k] = bf(low[:, pl.ds(to, LANES)])
    at = pl.multiple_of((z * TP_COUNT + core) * LANES, LANES)
    new, old = iota((count, rows), 0), iota((count, rows), 1)
    pick = hot(old == lax.div(new, seqs) * (Y_COUNT * seqs) + y * seqs + lax.rem(new, seqs))
    slab[...] = matmul(pick, xt[pl.ds(at, LANES), :], NT)


def load_mix(a0, a1, a2, a3, w_mix, sems):
    _, y, _ = place()
    moves = []
    for k, part in enumerate((a0, a1, a2, a3)):
        to = lax.rem(y - k + Y_COUNT, Y_COUNT)
        moves.append(
            pltpu.make_async_copy(
                part.at[pl.ds(LANES, w_mix.shape[1])], w_mix.at[to], sems.at[k]
            )
        )
    for move in moves:
        move.start()
    for move in moves:
        move.wait()


def load_state(state, held, sem):
    move = pltpu.make_async_copy(state, held, sem)
    move.start()
    move.wait()


def load_parts(*refs):
    *parts, held, sems = refs
    moves = [
        pltpu.make_async_copy(part.at[pl.ds(0, held.shape[1])], held.at[k], sems.at[k])
        for k, part in enumerate(parts)
    ]
    for move in moves:
        move.start()
    for move in moves:
        move.wait()


def flipped(x, out):
    out[...] = x[...].T


def assemble(tiles, rows):
    count = tiles.shape[0]
    for k in range(count):
        rows[:, k * LANES : (k + 1) * LANES] = tiles[k]


def normed_of(rows, gain):
    values = f32(rows[...])
    scale = lax.rsqrt(jnp.mean(values * values, axis=1, keepdims=True) + EPS)
    return bf(values * scale * gain[...])


def projections(tiles, gain, w_held, a3, channels, residual, rows, weights, sems):
    z, y, core = place()
    last = pltpu.make_async_copy(a3.at[pl.ds(0, LANES)], weights, sems.at[0])
    last.start()
    assemble(tiles, rows)
    normed = normed_of(rows, gain)
    flats = []
    for k in range(Y_COUNT - 1):
        flats.append(bf(matmul(normed, w_held[k], NT)))
    last.wait()
    flats.append(bf(matmul(normed, weights[...], NT)))
    count = rows.shape[0]
    seqs = count // Z_COUNT
    stacked = jnp.concatenate(flats, axis=0)
    shape = (Z_COUNT * 16, Y_COUNT * count)
    new, old = iota(shape, 0), iota(shape, 1)
    row = lax.div(new, 16) * seqs + lax.div(lax.rem(new, 16), Y_COUNT)
    wanted = lax.rem(y - lax.rem(new, Y_COUNT) + Y_COUNT, Y_COUNT) * count + row
    real = lax.div(lax.rem(new, 16), Y_COUNT) < seqs
    channels[...] = bf(matmul(hot((old == wanted) & real), stacked, NN))
    at = pl.multiple_of(z * TP_COUNT * LANES, 2 * LANES)
    both = rows[:, pl.ds(at, TP_COUNT * LANES)]
    shape = (TP_COUNT * LANES, LANES)
    old, new = iota(shape, 0), iota(shape, 1)
    each = LANES // Y_COUNT
    wanted = lax.div(new, each) * (TP_COUNT * each) + core * each + lax.rem(new, each)
    residual[...] = matmul(both, hot(old == wanted), NN)


def channel_views(arrived, k):
    per = LANES // KV_COUNT
    shape = (LANES, Z_COUNT * 16)
    channel, source = iota(shape, 0), iota(shape, 1)
    kv = lax.div(channel, per)
    wanted = lax.div(kv, Y_COUNT) * 16 + k * Y_COUNT + lax.rem(kv, Y_COUNT)
    wide = matmul(hot(source == wanted), arrived, NN)
    shape = (LANES, LANES)
    own = lax.rem(iota(shape, 0), per) == lax.rem(iota(shape, 1), per)
    wide = bf(jnp.where(own, wide, 0.0))
    shape = (LANES, KV_COUNT)
    gather = hot(lax.div(iota(shape, 0), per) == iota(shape, 1))
    shape = (KV_COUNT, LANES)
    gather_rows = hot(lax.div(iota(shape, 1), per) == iota(shape, 0))
    return matmul(wide, gather, NN), matmul(gather_rows, wide, NT)


def read_state(arrived, floor_rows, floor_t, gain, state, merged, vectors):
    seqs, heads = state.shape[:2]
    floor = floor_t[...]
    for k in range(seqs):
        columns, lines = channel_views(arrived[...], k)
        query = columns[:, :heads]
        raw = columns[:, heads : 2 * heads]
        forget = floor + (1.0 - floor) * jax.nn.sigmoid(raw)
        keep = (1.0 - floor) * jax.nn.sigmoid(-raw)
        line = lines[2 * heads : 3 * heads]
        raw = lines[heads : 2 * heads]
        low = floor_rows[...]
        vectors[k, :heads] = low + (1.0 - low) * jax.nn.sigmoid(raw)
        vectors[k, heads : 2 * heads] = (1.0 - low) * jax.nn.sigmoid(-raw)
        vectors[k, 2 * heads :] = line
        weight = query * forget
        added = jnp.sum(query * keep, axis=0, keepdims=True)
        outs = []
        for h in range(heads):
            term = weight[:, h : h + 1] * state[k, h]
            outs.append(
                jnp.sum(term, axis=0, keepdims=True) + added[:, h : h + 1] * line[h : h + 1]
            )
        readout = jnp.concatenate(outs, axis=0)
        scale = lax.rsqrt(jnp.mean(readout * readout, axis=1, keepdims=True) + EPS)
        gated = readout * scale * gain[...] * jax.nn.silu(lines[3 * heads : 4 * heads])
        merged[k * heads : (k + 1) * heads, :] = gated


def next_state(state, vectors, out):
    heads = out.shape[1]
    columns = vectors[0].T
    for h in range(heads):
        line = vectors[0, 2 * heads + h : 2 * heads + h + 1, :]
        out[0, h] = (
            columns[:, h : h + 1] * state[0, h] + columns[:, heads + h : heads + h + 1] * line
        )


def mix_out(tiles, w_mix, residual, after, rows):
    _, heads_rows, _ = tiles.shape
    slab_rows = rows.shape[0]
    seqs = slab_rows // Z_COUNT
    heads = heads_rows // seqs
    total = Z_COUNT * heads_rows
    shape = (total, total)
    new, old = iota(shape, 0), iota(shape, 1)
    row = lax.rem(new, slab_rows)
    wanted = (
        lax.div(row, seqs) * heads_rows + lax.rem(row, seqs) * heads + lax.div(new, slab_rows)
    )
    order = hot(old == wanted)
    for t in range(TP_COUNT):
        stacked = jnp.concatenate([tiles[z * TP_COUNT + t] for z in range(Z_COUNT)], axis=0)
        moved = bf(matmul(order, stacked, NN))
        for h in range(heads):
            at = (t * heads + h) * LANES
            rows[:, at : at + LANES] = moved[h * slab_rows : (h + 1) * slab_rows]
    weights = w_mix[...].reshape(LANES, rows.shape[1])
    after[...] = bf(residual[...] + matmul(rows[...], weights, NT))


def lane_order(transposed):
    shape = (TP_COUNT * LANES, TP_COUNT * LANES)
    each = LANES // Y_COUNT
    a, b = (0, 1) if not transposed else (1, 0)
    old, new = iota(shape, a), iota(shape, b)
    wanted = (
        lax.rem(lax.div(new, each), TP_COUNT) * LANES
        + lax.div(new, TP_COUNT * each) * each
        + lax.rem(new, each)
    )
    return hot(old == wanted)


def second_block(
    tiles, gain, after, w_held, t3, d0, d1, d2, d3, mine, theirs, rows, w_last, w_down, sems
):
    z, _, core = place()
    moves = [
        pltpu.make_async_copy(part, w_down.at[k], sems.at[k])
        for k, part in enumerate((d0, d1, d2, d3))
    ]
    last = pltpu.make_async_copy(t3, w_last, sems.at[Y_COUNT])
    last.start()
    for move in moves:
        move.start()
    order = lane_order(False)
    wide = TP_COUNT * LANES
    for k in range(Z_COUNT):
        both = jnp.concatenate([tiles[k * TP_COUNT], tiles[k * TP_COUNT + 1]], axis=1)
        rows[:, k * wide : (k + 1) * wide] = bf(matmul(both, order, NN))
    normed = normed_of(rows, gain)
    hidden = w_down.shape[1]
    mids = []
    for k in range(Y_COUNT):
        if k == Y_COUNT - 1:
            last.wait()
            w_top = w_last[...]
        else:
            w_top = w_held[k]
        tops = matmul(normed, w_top, NT)
        mids.append(bf(jax.nn.silu(tops[:, :hidden]) * tops[:, hidden:]))
    total = jnp.zeros(rows.shape, jnp.float32)
    for k, move in enumerate(moves):
        move.wait()
        total += matmul(mids[k], w_down[k], NN)
    total = bf(0.5 * total)
    back = lane_order(True)
    for k in range(Z_COUNT):
        split = matmul(total[:, k * wide : (k + 1) * wide], back, NN)
        low, high = split[:, :LANES], split[:, LANES:]
        kept = jnp.where(core == 0, low, high)
        home = jnp.where(z == k, f32(after[...]), 0.0)
        mine[k] = kept + home
        theirs[k] = bf(jnp.where(core == 0, high, low))


def finish(arrived, out):
    _, y, _ = place()
    slab_rows = arrived.shape[1]
    cols, rows = out.shape
    seqs = slab_rows // Z_COUNT
    parts = []
    for k in range(Y_COUNT):
        part = f32(arrived[k])
        for n in range(1, Z_COUNT):
            part += f32(arrived[n * Y_COUNT + k])
        parts.append(bf(part))
    result = jnp.concatenate(parts, axis=0)
    shape = (cols, LANES)
    pick = hot(iota(shape, 1) == y * cols + iota(shape, 0))
    picked = bf(matmul(pick, result, NT))
    shape = (rows, rows)
    old, new = iota(shape, 0), iota(shape, 1)
    wanted = (
        lax.rem(lax.div(new, seqs), Y_COUNT) * slab_rows
        + lax.div(new, seqs * Y_COUNT) * seqs
        + lax.rem(new, seqs)
    )
    out[...] = bf(matmul(picked, hot(old == wanted), NN))


def along_y(w):
    below, above = shift_y(w, 1), shift_y(w, -1)
    return below, above


def shards(
    hidden_in,
    state,
    forget_floor,
    ffn_gain_one,
    w_gate_one,
    w_up_one,
    w_down_one,
    mix_gain,
    w_query,
    w_forget,
    w_input,
    w_outgate,
    head_gain,
    w_mix_out,
    ffn_gain_two,
    w_gate_two,
    w_up_two,
    w_down_two,
):
    rows, own_cols = hidden_in.shape
    width, hidden = w_gate_one.shape
    seqs, heads = state.shape[:2]
    slab_rows = rows // Y_COUNT
    half16, half32 = jnp.bfloat16, jnp.float32
    dma = pltpu.SemaphoreType.DMA

    kinds = [jnp.transpose(w, (1, 2, 0)) for w in (w_query, w_forget, w_input, w_outgate)]
    early = jnp.concatenate([*(k.reshape(-1, width) for k in kinds), w_mix_out.T], axis=0)
    late_top = jnp.concatenate([w_gate_two.T, w_up_two.T], axis=0)

    (floor_t,) = local(flipped, [((LANES, heads), half32)], forget_floor)

    own = exchange(copies(hidden_in.T, KV_COUNT), "kv")
    other = swap_cores(own)
    mine, theirs, slab = local(
        first_block,
        [
            ((Z_COUNT, rows, LANES), half32),
            ((Z_COUNT, rows, LANES), half16),
            ((slab_rows, LANES), half32),
        ],
        own,
        other,
        ffn_gain_one.reshape(-1, LANES),
        w_gate_one.T,
        w_up_one.T,
        w_down_one,
        scratch=(
            pltpu.VMEM((width, rows), half16),
            pltpu.VMEM((rows, width), half32),
            pltpu.VMEM((hidden, width), half16),
            pltpu.VMEM((hidden, width), half16),
            pltpu.VMEM((hidden, width), half16),
            dma((3,)),
        ),
        outside=(3, 4, 5),
    )
    both = bf(mine + f32(swap_cores(theirs)))
    summed = exchange(both.reshape(KV_COUNT, slab_rows, LANES), "kv")
    below, above = shift_y(early, 1), shift_y(early, -1)
    twice = shift_y(below, 1)
    after_own = bf(slab + 0.5 * f32(summed).sum(axis=0))

    tops = [late_top, *along_y(late_top)]
    lows = [w_down_two, *along_y(w_down_two)]
    tops.append(shift_y(tops[1], 1))
    lows.append(shift_y(lows[2], -1))

    after_tiles = slab_exchange(after_own)
    parts = (early, below, twice, above)
    (w_held,) = local(
        load_parts,
        [((Y_COUNT - 1, LANES, width), half16)],
        *parts[:-1],
        scratch=(dma((Y_COUNT - 1,)),),
        outside=(0, 1, 2),
        vmem=True,
    )
    channels, residual = local(
        projections,
        [((Z_COUNT * 16, LANES), half16), ((slab_rows, LANES), half32)],
        after_tiles,
        mix_gain.reshape(1, -1),
        w_held,
        parts[-1],
        scratch=(
            pltpu.VMEM((slab_rows, width), half16),
            pltpu.VMEM((LANES, width), half16),
            dma((1,)),
        ),
        outside=(3,),
    )
    zgroups = [[a * Y_COUNT + b for a in range(Z_COUNT)] for b in range(Y_COUNT)]
    arrived = exchange(channels.reshape(Z_COUNT, 16, LANES), "kv", zgroups)
    (held,) = local(
        load_state,
        [(state.shape, half32)],
        state,
        scratch=(dma,),
        outside=(0,),
        vmem=True,
    )
    gated, vectors = local(
        read_state,
        [((seqs * heads, LANES), half32), ((seqs, 3 * heads, LANES), half32)],
        arrived.reshape(Z_COUNT * 16, LANES),
        forget_floor,
        floor_t,
        head_gain,
        held,
    )
    merged_tiles = slab_exchange(bf(gated))
    whole = lambda *dims: pl.BlockSpec((1, *dims), lambda k: (k, *(0 for _ in dims)))
    new_state = pl.pallas_call(
        next_state,
        grid=(seqs,),
        out_shape=jax.ShapeDtypeStruct(state.shape, half32),
        in_specs=[
            whole(*state.shape[1:]),
            whole(3 * heads, LANES),
        ],
        out_specs=whole(*state.shape[1:]),
        compiler_params=pltpu.CompilerParams(vmem_limit_bytes=VMEM_LIMIT),
        cost_estimate=pl.CostEstimate(flops=1 << 20, bytes_accessed=1 << 22, transcendentals=0),
        name="next_state",
    )(held, vectors)
    (w_mix,) = local(
        load_mix,
        [((Y_COUNT, own_cols, width), half16)],
        *parts,
        scratch=(dma((Y_COUNT,)),),
        outside=(0, 1, 2, 3),
        vmem=True,
    )
    (after_mix,) = local(
        mix_out,
        [((slab_rows, LANES), half16)],
        merged_tiles,
        w_mix,
        residual,
        scratch=(pltpu.VMEM((slab_rows, width), half16),),
    )

    mix_tiles = slab_exchange(after_mix)
    (w_held,) = local(
        load_parts,
        [((Y_COUNT - 1, 2 * hidden, width), half16)],
        *tops[:-1],
        scratch=(dma((Y_COUNT - 1,)),),
        outside=(0, 1, 2),
        vmem=True,
    )
    mine, theirs = local(
        second_block,
        [((Z_COUNT, slab_rows, LANES), half32), ((Z_COUNT, slab_rows, LANES), half16)],
        mix_tiles,
        ffn_gain_two.reshape(1, -1),
        after_mix,
        w_held,
        tops[-1],
        *lows,
        scratch=(
            pltpu.VMEM((slab_rows, width), half16),
            pltpu.VMEM((2 * hidden, width), half16),
            pltpu.VMEM((Y_COUNT, hidden, width), half16),
            dma((Y_COUNT + 1,)),
        ),
        outside=(4, 5, 6, 7, 8),
    )
    both = bf(mine + f32(swap_cores(theirs)))
    tiles = jnp.broadcast_to(both[:, None], (Z_COUNT, Y_COUNT, slab_rows, LANES))
    arrived = exchange(tiles.reshape(KV_COUNT, slab_rows, LANES), "kv")
    (result,) = local(finish, [((own_cols, rows), half16)], arrived)
    return (result.T, new_state)


def solution(mesh):
    return jax.shard_map(
        shards,
        mesh=mesh,
        in_specs=(
            P("dp", ("kv", "tp")),
            P(("dp", "kv"), "tp", None, None),
            P("tp", None),
            P(),
            P(None, ("kv", "tp")),
            P(None, ("kv", "tp")),
            P(("kv", "tp"), None),
            P(),
            P(None, "tp", "kv"),
            P(None, "tp", "kv"),
            P(None, "tp", "kv"),
            P(None, "tp", "kv"),
            P("tp", None),
            P(None, ("kv", "tp")),
            P(),
            P(None, ("kv", "tp")),
            P(None, ("kv", "tp")),
            P(("kv", "tp"), None),
        ),
        out_specs=(P("dp", ("kv", "tp")), P(("dp", "kv"), "tp", None, None)),
        check_vma=False,
    )
```

```python
import jax
import jax.numpy as jnp
from jax import lax
from jax.experimental import pallas as pl
from jax.experimental.pallas import tpu as pltpu
from jax.sharding import PartitionSpec as P

EPS = 1e-06
LANES = 128
Z_COUNT, Y_COUNT, TP_COUNT = 8, 4, 2
KV_COUNT = Z_COUNT * Y_COUNT
NN, NT = ((1,), (0,)), ((1,), (1,))


def bf(x):
    return x.astype(jnp.bfloat16)


def f32(x):
    return x.astype(jnp.float32)


def matmul(a, b, dims):
    return lax.dot_general(a, b, (dims, ((), ())), preferred_element_type=jnp.float32)


def exchange(tiles, axis, groups=None):
    return lax.all_to_all(
        tiles, axis, split_axis=0, concat_axis=0, axis_index_groups=groups, tiled=True
    )


def copies(x, count):
    return jnp.broadcast_to(x, (count, *x.shape))


def swap_cores(x):
    return lax.ppermute(x, "tp", [(0, 1), (1, 0)])


def shift_y(x, step):
    pairs = [
        (z * Y_COUNT + y, z * Y_COUNT + (y + step) % Y_COUNT)
        for z in range(Z_COUNT)
        for y in range(Y_COUNT)
    ]
    return lax.ppermute(x, "kv", pairs)


def slab_exchange(x):
    groups = [
        [(z * Y_COUNT + y) * TP_COUNT + t for z in range(Z_COUNT) for t in range(TP_COUNT)]
        for y in range(Y_COUNT)
    ]
    return exchange(copies(x, Z_COUNT * TP_COUNT), ("kv", "tp"), groups)


def place():
    kv = lax.axis_index("kv")
    return lax.div(kv, Y_COUNT), lax.rem(kv, Y_COUNT), lax.axis_index("tp")


def iota(shape, axis):
    return lax.broadcasted_iota(jnp.int32, shape, axis)


def hot(mask):
    return jnp.where(mask, 1.0, 0.0).astype(jnp.bfloat16)


def local(body, outs, *args, scratch=(), outside=(), held_out=False, vmem=False, flops=1 << 20):
    kind = pltpu.VMEM if vmem else jax.ShapeDtypeStruct
    shapes = [kind(s, d) for s, d in outs]
    held = pl.BlockSpec(memory_space=pltpu.VMEM)
    specs = [pl.BlockSpec(memory_space=pl.ANY) if k in outside else held for k in range(len(args))]
    args = [
        pltpu.with_memory_space_constraint(a, pltpu.HBM) if held_out and k in outside else a
        for k, a in enumerate(args)
    ]
    size = sum(a.size * a.dtype.itemsize for a in args)
    return pl.pallas_call(
        body,
        out_shape=shapes,
        in_specs=specs,
        out_specs=[held] * len(outs),
        scratch_shapes=list(scratch),
        compiler_params=pltpu.CompilerParams(vmem_limit_bytes=VMEM_LIMIT),
        cost_estimate=pl.CostEstimate(flops=flops, bytes_accessed=size, transcendentals=0),
    )(*args)


VMEM_LIMIT = 24 * 1024 * 1024


def first_block(
    own, other, gain, w_gate, w_up, w_down, mine, theirs, slab, xt, low, gate_w, up_w, down_w, sems
):
    z, y, core = place()
    moves = [
        pltpu.make_async_copy(src, dst, sems.at[k])
        for k, (src, dst) in enumerate(((w_gate, gate_w), (w_up, up_w), (w_down, down_w)))
    ]
    for move in moves:
        move.start()
    cols = own.shape[1]
    for kv in range(KV_COUNT):
        base = kv * TP_COUNT * cols
        xt[pl.ds(pl.multiple_of(base + core * cols, cols), cols), :] = own[kv]
        xt[pl.ds(pl.multiple_of(base + (1 - core) * cols, cols), cols), :] = other[kv]
    width, rows = xt.shape
    square = jnp.zeros((8, rows), jnp.float32)
    for c in range(width // LANES):
        part = f32(xt[c * LANES : (c + 1) * LANES, :])
        square += (part * part).reshape(LANES // 8, 8, rows).sum(axis=0)
    scale = lax.rsqrt(square.sum(axis=0, keepdims=True) * (1.0 / width) + EPS)
    gains = gain[...].T
    normed = []
    for c in range(width // LANES):
        part = f32(xt[c * LANES : (c + 1) * LANES, :])
        normed.append(bf(part * scale * gains[:, c : c + 1]))
    normed = jnp.concatenate(normed, axis=0)
    moves[0].wait()
    gate = matmul(gate_w[...], normed, NN)
    moves[1].wait()
    upper = matmul(up_w[...], normed, NN)
    mid = bf(jax.nn.silu(gate) * upper)
    count = slab.shape[0]
    seqs = count // Z_COUNT
    new, old = iota((rows, rows), 0), iota((rows, rows), 1)
    wanted = (
        lax.div(lax.rem(new, count), seqs) * (Y_COUNT * seqs)
        + lax.div(new, count) * seqs
        + lax.rem(new, seqs)
    )
    mid = bf(matmul(hot(old == wanted), mid, NT))
    moves[2].wait()
    low[...] = matmul(mid, down_w[...], NN)
    for k in range(Z_COUNT):
        at = pl.multiple_of((k * TP_COUNT + core) * LANES, LANES)
        to = pl.multiple_of((k * TP_COUNT + 1 - core) * LANES, LANES)
        mine[k] = low[:, pl.ds(at, LANES)]
        theirs[k] = bf(low[:, pl.ds(to, LANES)])
    at = pl.multiple_of((z * TP_COUNT + core) * LANES, LANES)
    new, old = iota((count, rows), 0), iota((count, rows), 1)
    pick = hot(old == lax.div(new, seqs) * (Y_COUNT * seqs) + y * seqs + lax.rem(new, seqs))
    slab[...] = matmul(pick, xt[pl.ds(at, LANES), :], NT)


def load_mix(a0, a1, a2, a3, w_mix, sems):
    _, y, _ = place()
    moves = []
    for k, part in enumerate((a0, a1, a2, a3)):
        to = lax.rem(y - k + Y_COUNT, Y_COUNT)
        moves.append(
            pltpu.make_async_copy(
                part.at[pl.ds(LANES, w_mix.shape[1])], w_mix.at[to], sems.at[k]
            )
        )
    for move in moves:
        move.start()
    for move in moves:
        move.wait()


def load_state(state, held, sem):
    move = pltpu.make_async_copy(state, held, sem)
    move.start()
    move.wait()


def load_parts(*refs):
    *parts, held, sems = refs
    moves = [
        pltpu.make_async_copy(part.at[pl.ds(0, held.shape[1])], held.at[k], sems.at[k])
        for k, part in enumerate(parts)
    ]
    for move in moves:
        move.start()
    for move in moves:
        move.wait()


def flipped(x, out):
    out[...] = x[...].T


def assemble(tiles, rows):
    count = tiles.shape[0]
    for k in range(count):
        rows[:, k * LANES : (k + 1) * LANES] = tiles[k]


def normed_of(rows, gain):
    values = f32(rows[...])
    scale = lax.rsqrt(jnp.mean(values * values, axis=1, keepdims=True) + EPS)
    return bf(values * scale * gain[...])


def projections(tiles, gain, w_held, a3, channels, residual, rows, weights, sems):
    z, y, core = place()
    last = pltpu.make_async_copy(a3.at[pl.ds(0, LANES)], weights, sems.at[0])
    last.start()
    assemble(tiles, rows)
    normed = normed_of(rows, gain)
    flats = []
    for k in range(Y_COUNT - 1):
        flats.append(bf(matmul(normed, w_held[k], NT)))
    last.wait()
    flats.append(bf(matmul(normed, weights[...], NT)))
    count = rows.shape[0]
    seqs = count // Z_COUNT
    stacked = jnp.concatenate(flats, axis=0)
    shape = (Z_COUNT * 16, Y_COUNT * count)
    new, old = iota(shape, 0), iota(shape, 1)
    row = lax.div(new, 16) * seqs + lax.div(lax.rem(new, 16), Y_COUNT)
    wanted = lax.rem(y - lax.rem(new, Y_COUNT) + Y_COUNT, Y_COUNT) * count + row
    real = lax.div(lax.rem(new, 16), Y_COUNT) < seqs
    channels[...] = bf(matmul(hot((old == wanted) & real), stacked, NN))
    at = pl.multiple_of(z * TP_COUNT * LANES, 2 * LANES)
    both = rows[:, pl.ds(at, TP_COUNT * LANES)]
    shape = (TP_COUNT * LANES, LANES)
    old, new = iota(shape, 0), iota(shape, 1)
    each = LANES // Y_COUNT
    wanted = lax.div(new, each) * (TP_COUNT * each) + core * each + lax.rem(new, each)
    residual[...] = matmul(both, hot(old == wanted), NN)


def channel_views(arrived, k):
    per = LANES // KV_COUNT
    shape = (LANES, Z_COUNT * 16)
    channel, source = iota(shape, 0), iota(shape, 1)
    kv = lax.div(channel, per)
    wanted = lax.div(kv, Y_COUNT) * 16 + k * Y_COUNT + lax.rem(kv, Y_COUNT)
    wide = matmul(hot(source == wanted), arrived, NN)
    shape = (LANES, LANES)
    own = lax.rem(iota(shape, 0), per) == lax.rem(iota(shape, 1), per)
    wide = bf(jnp.where(own, wide, 0.0))
    shape = (LANES, KV_COUNT)
    gather = hot(lax.div(iota(shape, 0), per) == iota(shape, 1))
    shape = (KV_COUNT, LANES)
    gather_rows = hot(lax.div(iota(shape, 1), per) == iota(shape, 0))
    return matmul(wide, gather, NN), matmul(gather_rows, wide, NT)


def read_state(arrived, floor_rows, floor_t, gain, state, merged, vectors):
    seqs, heads = state.shape[:2]
    floor = floor_t[...]
    for k in range(seqs):
        columns, lines = channel_views(arrived[...], k)
        query = columns[:, :heads]
        raw = columns[:, heads : 2 * heads]
        forget = floor + (1.0 - floor) * jax.nn.sigmoid(raw)
        keep = (1.0 - floor) * jax.nn.sigmoid(-raw)
        line = lines[2 * heads : 3 * heads]
        raw = lines[heads : 2 * heads]
        low = floor_rows[...]
        vectors[k, :heads] = low + (1.0 - low) * jax.nn.sigmoid(raw)
        vectors[k, heads : 2 * heads] = (1.0 - low) * jax.nn.sigmoid(-raw)
        vectors[k, 2 * heads :] = line
        weight = query * forget
        added = jnp.sum(query * keep, axis=0, keepdims=True)
        outs = []
        for h in range(heads):
            term = weight[:, h : h + 1] * state[k, h]
            outs.append(
                jnp.sum(term, axis=0, keepdims=True) + added[:, h : h + 1] * line[h : h + 1]
            )
        readout = jnp.concatenate(outs, axis=0)
        scale = lax.rsqrt(jnp.mean(readout * readout, axis=1, keepdims=True) + EPS)
        gated = readout * scale * gain[...] * jax.nn.silu(lines[3 * heads : 4 * heads])
        merged[k * heads : (k + 1) * heads, :] = gated


def next_state(state, vectors, out):
    heads = out.shape[1]
    columns = vectors[0].T
    for h in range(heads):
        line = vectors[0, 2 * heads + h : 2 * heads + h + 1, :]
        out[0, h] = (
            columns[:, h : h + 1] * state[0, h] + columns[:, heads + h : heads + h + 1] * line
        )


def mix_out(tiles, w_mix, residual, after, rows):
    _, heads_rows, _ = tiles.shape
    slab_rows = rows.shape[0]
    seqs = slab_rows // Z_COUNT
    heads = heads_rows // seqs
    total = Z_COUNT * heads_rows
    shape = (total, total)
    new, old = iota(shape, 0), iota(shape, 1)
    row = lax.rem(new, slab_rows)
    wanted = (
        lax.div(row, seqs) * heads_rows + lax.rem(row, seqs) * heads + lax.div(new, slab_rows)
    )
    order = hot(old == wanted)
    for t in range(TP_COUNT):
        stacked = jnp.concatenate([tiles[z * TP_COUNT + t] for z in range(Z_COUNT)], axis=0)
        moved = bf(matmul(order, stacked, NN))
        for h in range(heads):
            at = (t * heads + h) * LANES
            rows[:, at : at + LANES] = moved[h * slab_rows : (h + 1) * slab_rows]
    weights = w_mix[...].reshape(LANES, rows.shape[1])
    after[...] = bf(residual[...] + matmul(rows[...], weights, NT))


def lane_order(transposed):
    shape = (TP_COUNT * LANES, TP_COUNT * LANES)
    each = LANES // Y_COUNT
    a, b = (0, 1) if not transposed else (1, 0)
    old, new = iota(shape, a), iota(shape, b)
    wanted = (
        lax.rem(lax.div(new, each), TP_COUNT) * LANES
        + lax.div(new, TP_COUNT * each) * each
        + lax.rem(new, each)
    )
    return hot(old == wanted)


def second_block(
    tiles, gain, after, w_held, t3, d0, d1, d2, d3, mine, theirs, rows, w_last, w_down, sems
):
    z, _, core = place()
    moves = [
        pltpu.make_async_copy(part, w_down.at[k], sems.at[k])
        for k, part in enumerate((d0, d1, d2, d3))
    ]
    last = pltpu.make_async_copy(t3, w_last, sems.at[Y_COUNT])
    last.start()
    for move in moves:
        move.start()
    order = lane_order(False)
    wide = TP_COUNT * LANES
    for k in range(Z_COUNT):
        both = jnp.concatenate([tiles[k * TP_COUNT], tiles[k * TP_COUNT + 1]], axis=1)
        rows[:, k * wide : (k + 1) * wide] = bf(matmul(both, order, NN))
    normed = normed_of(rows, gain)
    hidden = w_down.shape[1]
    mids = []
    for k in range(Y_COUNT):
        if k == Y_COUNT - 1:
            last.wait()
            w_top = w_last[...]
        else:
            w_top = w_held[k]
        tops = matmul(normed, w_top, NT)
        mids.append(bf(jax.nn.silu(tops[:, :hidden]) * tops[:, hidden:]))
    total = jnp.zeros(rows.shape, jnp.float32)
    for k, move in enumerate(moves):
        move.wait()
        total += matmul(mids[k], w_down[k], NN)
    total = bf(0.5 * total)
    back = lane_order(True)
    for k in range(Z_COUNT):
        split = matmul(total[:, k * wide : (k + 1) * wide], back, NN)
        low, high = split[:, :LANES], split[:, LANES:]
        kept = jnp.where(core == 0, low, high)
        home = jnp.where(z == k, f32(after[...]), 0.0)
        mine[k] = kept + home
        theirs[k] = bf(jnp.where(core == 0, high, low))


def finish(arrived, out):
    _, y, _ = place()
    slab_rows = arrived.shape[1]
    cols, rows = out.shape
    seqs = slab_rows // Z_COUNT
    parts = []
    for k in range(Y_COUNT):
        part = f32(arrived[k])
        for n in range(1, Z_COUNT):
            part += f32(arrived[n * Y_COUNT + k])
        parts.append(bf(part))
    result = jnp.concatenate(parts, axis=0)
    shape = (cols, LANES)
    pick = hot(iota(shape, 1) == y * cols + iota(shape, 0))
    picked = bf(matmul(pick, result, NT))
    shape = (rows, rows)
    old, new = iota(shape, 0), iota(shape, 1)
    wanted = (
        lax.rem(lax.div(new, seqs), Y_COUNT) * slab_rows
        + lax.div(new, seqs * Y_COUNT) * seqs
        + lax.rem(new, seqs)
    )
    out[...] = bf(matmul(picked, hot(old == wanted), NN))


def shards(
    hidden_in,
    state,
    forget_floor,
    ffn_gain_one,
    w_gate_one,
    w_up_one,
    w_down_one,
    mix_gain,
    w_query,
    w_forget,
    w_input,
    w_outgate,
    head_gain,
    w_mix_out,
    ffn_gain_two,
    w_gate_two,
    w_up_two,
    w_down_two,
):
    rows, own_cols = hidden_in.shape
    width, hidden = w_gate_one.shape
    seqs, heads = state.shape[:2]
    slab_rows = rows // Y_COUNT
    half16, half32 = jnp.bfloat16, jnp.float32
    dma = pltpu.SemaphoreType.DMA

    kinds = [jnp.transpose(w, (1, 2, 0)) for w in (w_query, w_forget, w_input, w_outgate)]
    early = jnp.concatenate([*(k.reshape(-1, width) for k in kinds), w_mix_out.T], axis=0)
    late_top = jnp.concatenate([w_gate_two.T, w_up_two.T], axis=0)

    (floor_t,) = local(flipped, [((LANES, heads), half32)], forget_floor)

    own = exchange(copies(hidden_in.T, KV_COUNT), "kv")
    other = swap_cores(own)
    mine, theirs, slab = local(
        first_block,
        [
            ((Z_COUNT, rows, LANES), half32),
            ((Z_COUNT, rows, LANES), half16),
            ((slab_rows, LANES), half32),
        ],
        own,
        other,
        ffn_gain_one.reshape(-1, LANES),
        w_gate_one.T,
        w_up_one.T,
        w_down_one,
        scratch=(
            pltpu.VMEM((width, rows), half16),
            pltpu.VMEM((rows, width), half32),
            pltpu.VMEM((hidden, width), half16),
            pltpu.VMEM((hidden, width), half16),
            pltpu.VMEM((hidden, width), half16),
            dma((3,)),
        ),
        outside=(3, 4, 5),
        held_out=True,
    )
    both = bf(mine + f32(swap_cores(theirs)))
    summed = exchange(both.reshape(KV_COUNT, slab_rows, LANES), "kv")
    below, above = shift_y(early, 1), shift_y(early, -1)
    twice = shift_y(below, 1)
    after_own = bf(slab + 0.5 * f32(summed).sum(axis=0))

    top_above = shift_y(late_top, -1)
    top_below = shift_y(late_top, 1)
    low_above = shift_y(w_down_two, -1)
    low_below = shift_y(w_down_two, 1)
    top_far = shift_y(top_above, -1)
    low_far = shift_y(low_above, -1)
    tops = (late_top, top_below, top_above, top_far)
    lows = (w_down_two, low_below, low_above, low_far)

    after_tiles = slab_exchange(after_own)
    parts = (early, below, twice, above)
    (w_held,) = local(
        load_parts,
        [((Y_COUNT - 1, LANES, width), half16)],
        *parts[:-1],
        scratch=(dma((Y_COUNT - 1,)),),
        outside=(0, 1, 2),
        held_out=True,
        vmem=True,
    )
    channels, residual = local(
        projections,
        [((Z_COUNT * 16, LANES), half16), ((slab_rows, LANES), half32)],
        after_tiles,
        mix_gain.reshape(1, -1),
        w_held,
        parts[-1],
        scratch=(
            pltpu.VMEM((slab_rows, width), half16),
            pltpu.VMEM((LANES, width), half16),
            dma((1,)),
        ),
        outside=(3,),
        held_out=True,
    )
    zgroups = [[a * Y_COUNT + b for a in range(Z_COUNT)] for b in range(Y_COUNT)]
    arrived = exchange(channels.reshape(Z_COUNT, 16, LANES), "kv", zgroups)
    (held,) = local(
        load_state,
        [(state.shape, half32)],
        state,
        scratch=(dma,),
        outside=(0,),
        vmem=True,
    )
    gated, vectors = local(
        read_state,
        [((seqs * heads, LANES), half32), ((seqs, 3 * heads, LANES), half32)],
        arrived.reshape(Z_COUNT * 16, LANES),
        forget_floor,
        floor_t,
        head_gain,
        held,
    )
    merged_tiles = slab_exchange(bf(gated))
    whole = lambda *dims: pl.BlockSpec((1, *dims), lambda k: (k, *(0 for _ in dims)))
    new_state = pl.pallas_call(
        next_state,
        grid=(seqs,),
        out_shape=jax.ShapeDtypeStruct(state.shape, half32),
        in_specs=[
            whole(*state.shape[1:]),
            whole(3 * heads, LANES),
        ],
        out_specs=whole(*state.shape[1:]),
        compiler_params=pltpu.CompilerParams(vmem_limit_bytes=VMEM_LIMIT),
        cost_estimate=pl.CostEstimate(flops=1 << 20, bytes_accessed=1 << 22, transcendentals=0),
        name="next_state",
    )(held, vectors)
    (w_mix,) = local(
        load_mix,
        [((Y_COUNT, own_cols, width), half16)],
        *parts,
        scratch=(dma((Y_COUNT,)),),
        outside=(0, 1, 2, 3),
        held_out=True,
        vmem=True,
    )
    (after_mix,) = local(
        mix_out,
        [((slab_rows, LANES), half16)],
        merged_tiles,
        w_mix,
        residual,
        scratch=(pltpu.VMEM((slab_rows, width), half16),),
    )

    mix_tiles = slab_exchange(after_mix)
    (w_held,) = local(
        load_parts,
        [((Y_COUNT - 1, 2 * hidden, width), half16)],
        *tops[:-1],
        scratch=(dma((Y_COUNT - 1,)),),
        outside=(0, 1, 2),
        vmem=True,
    )
    mine, theirs = local(
        second_block,
        [((Z_COUNT, slab_rows, LANES), half32), ((Z_COUNT, slab_rows, LANES), half16)],
        mix_tiles,
        ffn_gain_two.reshape(1, -1),
        after_mix,
        w_held,
        tops[-1],
        *lows,
        scratch=(
            pltpu.VMEM((slab_rows, width), half16),
            pltpu.VMEM((2 * hidden, width), half16),
            pltpu.VMEM((Y_COUNT, hidden, width), half16),
            dma((Y_COUNT + 1,)),
        ),
        outside=(4, 5, 6, 7, 8),
    )
    both = bf(mine + f32(swap_cores(theirs)))
    tiles = jnp.broadcast_to(both[:, None], (Z_COUNT, Y_COUNT, slab_rows, LANES))
    arrived = exchange(tiles.reshape(KV_COUNT, slab_rows, LANES), "kv")
    (result,) = local(finish, [((own_cols, rows), half16)], arrived)
    return (result.T, new_state)


def solution(mesh):
    return jax.shard_map(
        shards,
        mesh=mesh,
        in_specs=(
            P("dp", ("kv", "tp")),
            P(("dp", "kv"), "tp", None, None),
            P("tp", None),
            P(),
            P(None, ("kv", "tp")),
            P(None, ("kv", "tp")),
            P(("kv", "tp"), None),
            P(),
            P(None, "tp", "kv"),
            P(None, "tp", "kv"),
            P(None, "tp", "kv"),
            P(None, "tp", "kv"),
            P("tp", None),
            P(None, ("kv", "tp")),
            P(),
            P(None, ("kv", "tp")),
            P(None, ("kv", "tp")),
            P(("kv", "tp"), None),
        ),
        out_specs=(P("dp", ("kv", "tp")), P(("dp", "kv"), "tp", None, None)),
        check_vma=False,
    )
```

```python
import jax
import jax.numpy as jnp
from jax import lax
from jax.experimental import pallas as pl
from jax.experimental.pallas import tpu as pltpu
from jax.sharding import PartitionSpec as P

EPS = 1e-06
LANES = 128
Z_COUNT, Y_COUNT, TP_COUNT = 8, 4, 2
KV_COUNT = Z_COUNT * Y_COUNT
NN, NT = ((1,), (0,)), ((1,), (1,))


def bf(x):
    return x.astype(jnp.bfloat16)


def f32(x):
    return x.astype(jnp.float32)


def matmul(a, b, dims):
    return lax.dot_general(a, b, (dims, ((), ())), preferred_element_type=jnp.float32)


def exchange(tiles, axis, groups=None):
    return lax.all_to_all(
        tiles, axis, split_axis=0, concat_axis=0, axis_index_groups=groups, tiled=True
    )


def copies(x, count):
    return jnp.broadcast_to(x, (count, *x.shape))


def swap_cores(x):
    return lax.ppermute(x, "tp", [(0, 1), (1, 0)])


def shift_y(x, step):
    pairs = [
        (z * Y_COUNT + y, z * Y_COUNT + (y + step) % Y_COUNT)
        for z in range(Z_COUNT)
        for y in range(Y_COUNT)
    ]
    return lax.ppermute(x, "kv", pairs)


def slab_exchange(x):
    groups = [
        [(z * Y_COUNT + y) * TP_COUNT + t for z in range(Z_COUNT) for t in range(TP_COUNT)]
        for y in range(Y_COUNT)
    ]
    return exchange(copies(x, Z_COUNT * TP_COUNT), ("kv", "tp"), groups)


def div(v, d):
    if d & (d - 1) == 0:
        return v >> (d.bit_length() - 1)
    return (v * (65536 // d + 1)) >> 16


def rem(v, d):
    return v & (d - 1) if d & (d - 1) == 0 else v - div(v, d) * d


def place():
    kv = lax.axis_index("kv")
    return div(kv, Y_COUNT), rem(kv, Y_COUNT), lax.axis_index("tp")


def iota(shape, axis):
    return lax.broadcasted_iota(jnp.int32, shape, axis)


def hot(mask):
    return jnp.where(mask, 1.0, 0.0).astype(jnp.bfloat16)


def local(body, outs, *args, scratch=(), outside=(), held_out=False, vmem=False, flops=1 << 20):
    kind = pltpu.VMEM if vmem else jax.ShapeDtypeStruct
    shapes = [kind(s, d) for s, d in outs]
    held = pl.BlockSpec(memory_space=pltpu.VMEM)
    specs = [pl.BlockSpec(memory_space=pl.ANY) if k in outside else held for k in range(len(args))]
    args = [
        pltpu.with_memory_space_constraint(a, pltpu.HBM) if held_out and k in outside else a
        for k, a in enumerate(args)
    ]
    size = sum(a.size * a.dtype.itemsize for a in args)
    return pl.pallas_call(
        body,
        out_shape=shapes,
        in_specs=specs,
        out_specs=[held] * len(outs),
        scratch_shapes=list(scratch),
        compiler_params=pltpu.CompilerParams(vmem_limit_bytes=VMEM_LIMIT),
        cost_estimate=pl.CostEstimate(flops=flops, bytes_accessed=size, transcendentals=0),
    )(*args)


VMEM_LIMIT = 24 * 1024 * 1024


def load_first(w_gate, w_up, w_down, gate, upper, down, sems):
    moves = [
        pltpu.make_async_copy(src, dst, sems.at[k])
        for k, (src, dst) in enumerate(((w_gate, gate), (w_up, upper), (w_down, down)))
    ]
    for move in moves:
        move.start()
    for move in moves:
        move.wait()


def first_block(own, other, gain, w_gate, w_up, w_down, mine, theirs, slab, xt, low):
    z, y, core = place()
    cols = own.shape[1]
    for kv in range(KV_COUNT):
        base = kv * TP_COUNT * cols
        xt[pl.ds(pl.multiple_of(base + core * cols, cols), cols), :] = own[kv]
        xt[pl.ds(pl.multiple_of(base + (1 - core) * cols, cols), cols), :] = other[kv]
    width, rows = xt.shape
    square = jnp.zeros((8, rows), jnp.float32)
    for c in range(width // LANES):
        part = f32(xt[c * LANES : (c + 1) * LANES, :])
        square += (part * part).reshape(LANES // 8, 8, rows).sum(axis=0)
    scale = lax.rsqrt(square.sum(axis=0, keepdims=True) * (1.0 / width) + EPS)
    gains = gain[...].T
    normed = []
    for c in range(width // LANES):
        part = f32(xt[c * LANES : (c + 1) * LANES, :])
        normed.append(bf(part * scale * gains[:, c : c + 1]))
    normed = jnp.concatenate(normed, axis=0)
    gate = matmul(w_gate[...], normed, NN)
    upper = matmul(w_up[...], normed, NN)
    mid = bf(jax.nn.silu(gate) * upper)
    count = slab.shape[0]
    seqs = count // Z_COUNT
    new, old = iota((rows, rows), 0), iota((rows, rows), 1)
    wanted = (
        div(rem(new, count), seqs) * (Y_COUNT * seqs)
        + div(new, count) * seqs
        + rem(new, seqs)
    )
    mid = bf(matmul(hot(old == wanted), mid, NT))
    low[...] = matmul(mid, w_down[...], NN)
    for k in range(Z_COUNT):
        at = pl.multiple_of((k * TP_COUNT + core) * LANES, LANES)
        to = pl.multiple_of((k * TP_COUNT + 1 - core) * LANES, LANES)
        mine[k] = low[:, pl.ds(at, LANES)]
        theirs[k] = bf(low[:, pl.ds(to, LANES)])
    at = pl.multiple_of((z * TP_COUNT + core) * LANES, LANES)
    new, old = iota((count, rows), 0), iota((count, rows), 1)
    pick = hot(old == div(new, seqs) * (Y_COUNT * seqs) + y * seqs + rem(new, seqs))
    slab[...] = matmul(pick, xt[pl.ds(at, LANES), :], NT)


def load_mix(a0, a1, a2, a3, w_mix, sems):
    _, y, _ = place()
    moves = []
    for k, part in enumerate((a0, a1, a2, a3)):
        to = rem(y - k + Y_COUNT, Y_COUNT)
        moves.append(
            pltpu.make_async_copy(
                part.at[pl.ds(LANES, w_mix.shape[1])], w_mix.at[to], sems.at[k]
            )
        )
    for move in moves:
        move.start()
    for move in moves:
        move.wait()


def load_state(state, held, sem):
    move = pltpu.make_async_copy(state, held, sem)
    move.start()
    move.wait()


def load_parts(*refs):
    *parts, held, sems = refs
    moves = [
        pltpu.make_async_copy(part.at[pl.ds(0, held.shape[1])], held.at[k], sems.at[k])
        for k, part in enumerate(parts)
    ]
    for move in moves:
        move.start()
    for move in moves:
        move.wait()


def pack_early(query, forget, inputs, out_gate, mix, out, *scratch):
    *held, sems = scratch
    moves = [
        pltpu.make_async_copy(w, held[k], sems.at[k])
        for k, w in enumerate((query, forget, inputs, out_gate))
    ]
    rest = out.shape[0] - LANES
    moves.append(pltpu.make_async_copy(mix, out.at[pl.ds(LANES, rest)], sems.at[4]))
    for move in moves:
        move.start()
    heads, per, _ = query.shape
    for k in range(4):
        moves[k].wait()
        for h in range(0, heads, 4):
            block = jnp.concatenate([f32(held[k][h + n]) for n in range(4)], axis=0)
            at = (k * heads + h) * per
            out[at : at + 4 * per, :] = bf(block)
    moves[4].wait()


def flipped(x, out):
    out[...] = x[...].T


def assemble(tiles, rows):
    count = tiles.shape[0]
    for k in range(count):
        rows[:, k * LANES : (k + 1) * LANES] = tiles[k]


def normed_of(rows, gain):
    values = f32(rows[...])
    scale = lax.rsqrt(jnp.mean(values * values, axis=1, keepdims=True) + EPS)
    return bf(values * scale * gain[...])


def projections(tiles, gain, w_held, a3, channels, residual, rows, weights, sems):
    z, y, core = place()
    last = pltpu.make_async_copy(a3.at[pl.ds(0, LANES)], weights, sems.at[0])
    last.start()
    assemble(tiles, rows)
    normed = normed_of(rows, gain)
    flats = []
    for k in range(Y_COUNT - 1):
        flats.append(bf(matmul(normed, w_held[k], NT)))
    last.wait()
    flats.append(bf(matmul(normed, weights[...], NT)))
    count = rows.shape[0]
    seqs = count // Z_COUNT
    stacked = jnp.concatenate(flats, axis=0)
    shape = (Z_COUNT * 16, Y_COUNT * count)
    new, old = iota(shape, 0), iota(shape, 1)
    row = div(new, 16) * seqs + div(rem(new, 16), Y_COUNT)
    wanted = rem(y - rem(new, Y_COUNT) + Y_COUNT, Y_COUNT) * count + row
    real = div(rem(new, 16), Y_COUNT) < seqs
    channels[...] = bf(matmul(hot((old == wanted) & real), stacked, NN))
    at = pl.multiple_of(z * TP_COUNT * LANES, 2 * LANES)
    both = rows[:, pl.ds(at, TP_COUNT * LANES)]
    shape = (TP_COUNT * LANES, LANES)
    old, new = iota(shape, 0), iota(shape, 1)
    each = LANES // Y_COUNT
    wanted = div(new, each) * (TP_COUNT * each) + core * each + rem(new, each)
    residual[...] = matmul(both, hot(old == wanted), NN)


def channel_views(arrived, k):
    per = LANES // KV_COUNT
    shape = (LANES, Z_COUNT * 16)
    channel, source = iota(shape, 0), iota(shape, 1)
    kv = div(channel, per)
    wanted = div(kv, Y_COUNT) * 16 + k * Y_COUNT + rem(kv, Y_COUNT)
    wide = matmul(hot(source == wanted), arrived, NN)
    shape = (LANES, LANES)
    own = rem(iota(shape, 0), per) == rem(iota(shape, 1), per)
    wide = bf(jnp.where(own, wide, 0.0))
    shape = (LANES, KV_COUNT)
    gather = hot(div(iota(shape, 0), per) == iota(shape, 1))
    shape = (KV_COUNT, LANES)
    gather_rows = hot(div(iota(shape, 1), per) == iota(shape, 0))
    return matmul(wide, gather, NN), matmul(gather_rows, wide, NT)


def read_state(arrived, floor_rows, floor_t, gain, state, merged, vectors):
    seqs, heads = state.shape[:2]
    floor = floor_t[...]
    for k in range(seqs):
        columns, lines = channel_views(arrived[...], k)
        query = columns[:, :heads]
        raw = columns[:, heads : 2 * heads]
        forget = floor + (1.0 - floor) * jax.nn.sigmoid(raw)
        keep = (1.0 - floor) * jax.nn.sigmoid(-raw)
        line = lines[2 * heads : 3 * heads]
        raw = lines[heads : 2 * heads]
        low = floor_rows[...]
        vectors[k, :heads] = low + (1.0 - low) * jax.nn.sigmoid(raw)
        vectors[k, heads : 2 * heads] = (1.0 - low) * jax.nn.sigmoid(-raw)
        vectors[k, 2 * heads :] = line
        weight = query * forget
        added = jnp.sum(query * keep, axis=0, keepdims=True)
        outs = []
        for h in range(heads):
            term = weight[:, h : h + 1] * state[k, h]
            outs.append(
                jnp.sum(term, axis=0, keepdims=True) + added[:, h : h + 1] * line[h : h + 1]
            )
        readout = jnp.concatenate(outs, axis=0)
        scale = lax.rsqrt(jnp.mean(readout * readout, axis=1, keepdims=True) + EPS)
        gated = readout * scale * gain[...] * jax.nn.silu(lines[3 * heads : 4 * heads])
        merged[k * heads : (k + 1) * heads, :] = gated


def next_state(state, vectors, out):
    heads = out.shape[1]
    columns = vectors[0].T
    for h in range(heads):
        line = vectors[0, 2 * heads + h : 2 * heads + h + 1, :]
        out[0, h] = (
            columns[:, h : h + 1] * state[0, h] + columns[:, heads + h : heads + h + 1] * line
        )


def mix_out(tiles, w_mix, residual, after, rows):
    _, heads_rows, _ = tiles.shape
    slab_rows = rows.shape[0]
    seqs = slab_rows // Z_COUNT
    heads = heads_rows // seqs
    total = Z_COUNT * heads_rows
    shape = (total, total)
    new, old = iota(shape, 0), iota(shape, 1)
    row = rem(new, slab_rows)
    wanted = (
        div(row, seqs) * heads_rows + rem(row, seqs) * heads + div(new, slab_rows)
    )
    order = hot(old == wanted)
    for t in range(TP_COUNT):
        stacked = jnp.concatenate([tiles[z * TP_COUNT + t] for z in range(Z_COUNT)], axis=0)
        moved = bf(matmul(order, stacked, NN))
        for h in range(heads):
            at = (t * heads + h) * LANES
            rows[:, at : at + LANES] = moved[h * slab_rows : (h + 1) * slab_rows]
    weights = w_mix[...].reshape(LANES, rows.shape[1])
    after[...] = bf(residual[...] + matmul(rows[...], weights, NT))


def lane_order(transposed):
    shape = (TP_COUNT * LANES, TP_COUNT * LANES)
    each = LANES // Y_COUNT
    a, b = (0, 1) if not transposed else (1, 0)
    old, new = iota(shape, a), iota(shape, b)
    wanted = (
        rem(div(new, each), TP_COUNT) * LANES
        + div(new, TP_COUNT * each) * each
        + rem(new, each)
    )
    return hot(old == wanted)


def second_block(
    tiles, gain, after, w_held, t3, d0, d1, d2, d3, out, rows, w_last, w_down, sems
):
    z, _, core = place()
    moves = [
        pltpu.make_async_copy(part, w_down.at[k], sems.at[k])
        for k, part in enumerate((d0, d1, d2, d3))
    ]
    last = pltpu.make_async_copy(t3, w_last, sems.at[Y_COUNT])
    last.start()
    for move in moves:
        move.start()
    order = lane_order(False)
    wide = TP_COUNT * LANES
    count = rows.shape[0]
    pairs = [
        jnp.concatenate([tiles[k * TP_COUNT], tiles[k * TP_COUNT + 1]], axis=1)
        for k in range(Z_COUNT)
    ]
    ordered = bf(matmul(jnp.concatenate(pairs, axis=0), order, NN))
    for k in range(Z_COUNT):
        rows[:, k * wide : (k + 1) * wide] = ordered[k * count : (k + 1) * count]
    normed = normed_of(rows, gain)
    hidden = w_down.shape[1]
    mids = []
    for k in range(Y_COUNT):
        if k == Y_COUNT - 1:
            last.wait()
            w_top = w_last[...]
        else:
            w_top = w_held[k]
        tops = matmul(normed, w_top, NT)
        mids.append(bf(jax.nn.silu(tops[:, :hidden]) * tops[:, hidden:]))
    total = jnp.zeros(rows.shape, jnp.float32)
    for k, move in enumerate(moves):
        move.wait()
        total += matmul(mids[k], w_down[k], NN)
    each = LANES // Y_COUNT
    total = 0.5 * total
    spare = jnp.zeros((each - count, LANES), jnp.float32)

    def spread(block):
        padded = jnp.concatenate([block, spare], axis=0)
        return jnp.concatenate([padded] * Y_COUNT, axis=0).T

    group = div(iota((8, LANES), 1), each)
    home = spread(f32(after[...]))
    for k in range(Z_COUNT * TP_COUNT):
        block = spread(total[:, k * LANES : (k + 1) * LANES])
        for n in range(Y_COUNT):
            where = rem(k, TP_COUNT) * Y_COUNT + n
            own_y, t = div(where, TP_COUNT), rem(where, TP_COUNT)
            packed = jnp.zeros((8, LANES), jnp.float32)
            extra = jnp.zeros((8, LANES), jnp.float32)
            for g in range(Y_COUNT):
                at, to = n * each + g * 8, own_y * each + g * 8
                packed = jnp.where(group == g, block[at : at + 8], packed)
                extra = jnp.where(group == g, home[to : to + 8], extra)
            own = (z == div(k, TP_COUNT)) & (core == t)
            packed = packed + jnp.where(own, extra, 0.0)
            out[(div(k, TP_COUNT) * Y_COUNT + own_y) * TP_COUNT + t] = bf(packed)


def finish(arrived, out):
    cols, rows = out.shape
    slab_rows = rows // Y_COUNT
    seqs = slab_rows // Z_COUNT
    lanes_each = LANES // Y_COUNT
    parts = []
    for k in range(Y_COUNT):
        part = jnp.zeros(arrived.shape[1:], jnp.float32)
        for n in range(Z_COUNT):
            for t in range(TP_COUNT):
                part += f32(arrived[(n * Y_COUNT + k) * TP_COUNT + t])
        parts.append(bf(part))
    sums = jnp.concatenate(parts, axis=1)
    shape = (Y_COUNT * LANES, rows)
    old, new = iota(shape, 0), iota(shape, 1)
    y = rem(div(new, seqs), Y_COUNT)
    row = div(new, seqs * Y_COUNT) * seqs + rem(new, seqs)
    for g in range(cols // 8):
        pick = hot(old == y * LANES + g * lanes_each + row)
        out[g * 8 : (g + 1) * 8, :] = bf(matmul(sums, pick, NN))


def shards(
    hidden_in,
    state,
    forget_floor,
    ffn_gain_one,
    w_gate_one,
    w_up_one,
    w_down_one,
    mix_gain,
    w_query,
    w_forget,
    w_input,
    w_outgate,
    head_gain,
    w_mix_out,
    ffn_gain_two,
    w_gate_two,
    w_up_two,
    w_down_two,
):
    rows, own_cols = hidden_in.shape
    width, hidden = w_gate_one.shape
    seqs, heads = state.shape[:2]
    slab_rows = rows // Y_COUNT
    half16, half32 = jnp.bfloat16, jnp.float32
    dma = pltpu.SemaphoreType.DMA

    kinds = [jnp.transpose(w, (1, 2, 0)) for w in (w_query, w_forget, w_input, w_outgate)]
    (early,) = local(
        pack_early,
        [((LANES + own_cols, width), half16)],
        *kinds,
        w_mix_out.T,
        scratch=(*[pltpu.VMEM(k.shape, half16) for k in kinds], dma((5,))),
        outside=(0, 1, 2, 3, 4),
        held_out=True,
    )
    late_top = jnp.concatenate([w_gate_two.T, w_up_two.T], axis=0)

    (floor_t,) = local(flipped, [((LANES, heads), half32)], forget_floor)

    own = exchange(copies(hidden_in.T, KV_COUNT), "kv")
    first_w = local(
        load_first,
        [((hidden, width), half16)] * 3,
        w_gate_one.T,
        w_up_one.T,
        w_down_one,
        scratch=(dma((3,)),),
        outside=(0, 1, 2),
        held_out=True,
        vmem=True,
    )
    other = swap_cores(own)
    mine, theirs, slab = local(
        first_block,
        [
            ((Z_COUNT, rows, LANES), half32),
            ((Z_COUNT, rows, LANES), half16),
            ((slab_rows, LANES), half32),
        ],
        own,
        other,
        ffn_gain_one.reshape(-1, LANES),
        *first_w,
        scratch=(pltpu.VMEM((width, rows), half16), pltpu.VMEM((rows, width), half32)),
    )
    both = bf(mine + f32(swap_cores(theirs)))
    summed = exchange(both.reshape(KV_COUNT, slab_rows, LANES), "kv")
    below, above = shift_y(early, 1), shift_y(early, -1)
    twice = shift_y(below, 1)
    after_own = bf(slab + 0.5 * f32(summed).sum(axis=0))

    top_above = shift_y(late_top, -1)
    top_below = shift_y(late_top, 1)
    low_above = shift_y(w_down_two, -1)
    low_below = shift_y(w_down_two, 1)
    top_far = shift_y(top_above, -1)
    low_far = shift_y(low_above, -1)
    tops = (late_top, top_below, top_above, top_far)
    lows = (w_down_two, low_below, low_above, low_far)

    after_tiles = slab_exchange(after_own)
    parts = (early, below, twice, above)
    (w_held,) = local(
        load_parts,
        [((Y_COUNT - 1, LANES, width), half16)],
        *parts[:-1],
        scratch=(dma((Y_COUNT - 1,)),),
        outside=(0, 1, 2),
        held_out=True,
        vmem=True,
    )
    channels, residual = local(
        projections,
        [((Z_COUNT * 16, LANES), half16), ((slab_rows, LANES), half32)],
        after_tiles,
        mix_gain.reshape(1, -1),
        w_held,
        parts[-1],
        scratch=(
            pltpu.VMEM((slab_rows, width), half16),
            pltpu.VMEM((LANES, width), half16),
            dma((1,)),
        ),
        outside=(3,),
        held_out=True,
    )
    zgroups = [[a * Y_COUNT + b for a in range(Z_COUNT)] for b in range(Y_COUNT)]
    arrived = exchange(channels.reshape(Z_COUNT, 16, LANES), "kv", zgroups)
    (held,) = local(
        load_state,
        [(state.shape, half32)],
        state,
        scratch=(dma,),
        outside=(0,),
        vmem=True,
    )
    gated, vectors = local(
        read_state,
        [((seqs * heads, LANES), half32), ((seqs, 3 * heads, LANES), half32)],
        arrived.reshape(Z_COUNT * 16, LANES),
        forget_floor,
        floor_t,
        head_gain,
        held,
    )
    merged_tiles = slab_exchange(bf(gated))
    whole = lambda *dims: pl.BlockSpec((1, *dims), lambda k: (k, *(0 for _ in dims)))
    new_state = pl.pallas_call(
        next_state,
        grid=(seqs,),
        out_shape=jax.ShapeDtypeStruct(state.shape, half32),
        in_specs=[
            whole(*state.shape[1:]),
            whole(3 * heads, LANES),
        ],
        out_specs=whole(*state.shape[1:]),
        compiler_params=pltpu.CompilerParams(vmem_limit_bytes=VMEM_LIMIT),
        cost_estimate=pl.CostEstimate(flops=1 << 20, bytes_accessed=1 << 22, transcendentals=0),
        name="next_state",
    )(held, vectors)
    (w_mix,) = local(
        load_mix,
        [((Y_COUNT, own_cols, width), half16)],
        *parts,
        scratch=(dma((Y_COUNT,)),),
        outside=(0, 1, 2, 3),
        held_out=True,
        vmem=True,
    )
    (after_mix,) = local(
        mix_out,
        [((slab_rows, LANES), half16)],
        merged_tiles,
        w_mix,
        residual,
        scratch=(pltpu.VMEM((slab_rows, width), half16),),
    )

    mix_tiles = slab_exchange(after_mix)
    (w_held,) = local(
        load_parts,
        [((Y_COUNT - 1, 2 * hidden, width), half16)],
        *tops[:-1],
        scratch=(dma((Y_COUNT - 1,)),),
        outside=(0, 1, 2),
        vmem=True,
    )
    (messages,) = local(
        second_block,
        [((KV_COUNT * TP_COUNT, 8, LANES), half16)],
        mix_tiles,
        ffn_gain_two.reshape(1, -1),
        after_mix,
        w_held,
        tops[-1],
        *lows,
        scratch=(
            pltpu.VMEM((slab_rows, width), half16),
            pltpu.VMEM((2 * hidden, width), half16),
            pltpu.VMEM((Y_COUNT, hidden, width), half16),
            dma((Y_COUNT + 1,)),
        ),
        outside=(4, 5, 6, 7, 8),
    )
    arrived = exchange(messages, ("kv", "tp"))
    (result,) = local(finish, [((own_cols, rows), half16)], arrived)
    return (result.T, new_state)


def solution(mesh):
    return jax.shard_map(
        shards,
        mesh=mesh,
        in_specs=(
            P("dp", ("kv", "tp")),
            P(("dp", "kv"), "tp", None, None),
            P("tp", None),
            P(),
            P(None, ("kv", "tp")),
            P(None, ("kv", "tp")),
            P(("kv", "tp"), None),
            P(),
            P(None, "tp", "kv"),
            P(None, "tp", "kv"),
            P(None, "tp", "kv"),
            P(None, "tp", "kv"),
            P("tp", None),
            P(None, ("kv", "tp")),
            P(),
            P(None, ("kv", "tp")),
            P(None, ("kv", "tp")),
            P(("kv", "tp"), None),
        ),
        out_specs=(P("dp", ("kv", "tp")), P(("dp", "kv"), "tp", None, None)),
        check_vma=False,
    )
```

```python
import jax
import jax.numpy as jnp
from jax import lax
from jax.experimental import pallas as pl
from jax.experimental.pallas import tpu as pltpu
from jax.sharding import PartitionSpec as P

EPS = 1e-06
LANES = 128
Z_COUNT, Y_COUNT, TP_COUNT = 8, 4, 2
KV_COUNT = Z_COUNT * Y_COUNT
NN, NT = ((1,), (0,)), ((1,), (1,))


def bf(x):
    return x.astype(jnp.bfloat16)


def f32(x):
    return x.astype(jnp.float32)


def matmul(a, b, dims):
    return lax.dot_general(a, b, (dims, ((), ())), preferred_element_type=jnp.float32)


def exchange(tiles, axis, groups=None):
    return lax.all_to_all(
        tiles, axis, split_axis=0, concat_axis=0, axis_index_groups=groups, tiled=True
    )


def copies(x, count):
    return jnp.broadcast_to(x, (count, *x.shape))


def swap_cores(x):
    return lax.ppermute(x, "tp", [(0, 1), (1, 0)])


def shift_y(x, step):
    pairs = [
        (z * Y_COUNT + y, z * Y_COUNT + (y + step) % Y_COUNT)
        for z in range(Z_COUNT)
        for y in range(Y_COUNT)
    ]
    return lax.ppermute(x, "kv", pairs)


def slab_exchange(x):
    groups = [
        [(z * Y_COUNT + y) * TP_COUNT + t for z in range(Z_COUNT) for t in range(TP_COUNT)]
        for y in range(Y_COUNT)
    ]
    return exchange(copies(x, Z_COUNT * TP_COUNT), ("kv", "tp"), groups)


def div(v, d):
    if d & (d - 1) == 0:
        return v >> (d.bit_length() - 1)
    return (v * (65536 // d + 1)) >> 16


def rem(v, d):
    return v & (d - 1) if d & (d - 1) == 0 else v - div(v, d) * d


def place():
    kv = lax.axis_index("kv")
    return div(kv, Y_COUNT), rem(kv, Y_COUNT), lax.axis_index("tp")


def iota(shape, axis):
    return lax.broadcasted_iota(jnp.int32, shape, axis)


def hot(mask):
    return jnp.where(mask, 1.0, 0.0).astype(jnp.bfloat16)


def local(body, outs, *args, scratch=(), outside=(), held_out=False, vmem=False, sent=(), flops=1 << 20):
    kind = pltpu.VMEM if vmem else jax.ShapeDtypeStruct
    shapes = [pltpu.HBM(s, d) if k in sent else kind(s, d) for k, (s, d) in enumerate(outs)]
    placed = [
        pl.BlockSpec(memory_space=pltpu.HBM) if k in sent else pl.BlockSpec(memory_space=pltpu.VMEM)
        for k in range(len(outs))
    ]
    held = pl.BlockSpec(memory_space=pltpu.VMEM)
    specs = [pl.BlockSpec(memory_space=pl.ANY) if k in outside else held for k in range(len(args))]
    args = [
        pltpu.with_memory_space_constraint(a, pltpu.HBM) if held_out and k in outside else a
        for k, a in enumerate(args)
    ]
    size = sum(a.size * a.dtype.itemsize for a in args)
    return pl.pallas_call(
        body,
        out_shape=shapes,
        in_specs=specs,
        out_specs=placed,
        scratch_shapes=list(scratch),
        compiler_params=pltpu.CompilerParams(vmem_limit_bytes=VMEM_LIMIT),
        cost_estimate=pl.CostEstimate(flops=flops, bytes_accessed=size, transcendentals=0),
    )(*args)


VMEM_LIMIT = 24 * 1024 * 1024


def load_first(w_gate, w_up, w_down, gate, upper, down, sems):
    moves = [
        pltpu.make_async_copy(src, dst, sems.at[k])
        for k, (src, dst) in enumerate(((w_gate, gate), (w_up, upper), (w_down, down)))
    ]
    for move in moves:
        move.start()
    for move in moves:
        move.wait()


def first_block(own, other, gain, w_gate, w_up, w_down, mine, theirs, slab, xt, low):
    z, y, core = place()
    cols = own.shape[1]
    for kv in range(KV_COUNT):
        base = kv * TP_COUNT * cols
        xt[pl.ds(pl.multiple_of(base + core * cols, cols), cols), :] = own[kv]
        xt[pl.ds(pl.multiple_of(base + (1 - core) * cols, cols), cols), :] = other[kv]
    width, rows = xt.shape
    square = jnp.zeros((8, rows), jnp.float32)
    for c in range(width // LANES):
        part = f32(xt[c * LANES : (c + 1) * LANES, :])
        square += (part * part).reshape(LANES // 8, 8, rows).sum(axis=0)
    scale = lax.rsqrt(square.sum(axis=0, keepdims=True) * (1.0 / width) + EPS)
    gains = gain[...].T
    normed = []
    for c in range(width // LANES):
        part = f32(xt[c * LANES : (c + 1) * LANES, :])
        normed.append(bf(part * scale * gains[:, c : c + 1]))
    normed = jnp.concatenate(normed, axis=0)
    gate = matmul(w_gate[...], normed, NN)
    upper = matmul(w_up[...], normed, NN)
    mid = bf(jax.nn.silu(gate) * upper)
    count = slab.shape[0]
    seqs = count // Z_COUNT
    new, old = iota((rows, rows), 0), iota((rows, rows), 1)
    wanted = (
        div(rem(new, count), seqs) * (Y_COUNT * seqs)
        + div(new, count) * seqs
        + rem(new, seqs)
    )
    mid = bf(matmul(hot(old == wanted), mid, NT))
    low[...] = matmul(mid, w_down[...], NN)
    for k in range(Z_COUNT):
        at = pl.multiple_of((k * TP_COUNT + core) * LANES, LANES)
        to = pl.multiple_of((k * TP_COUNT + 1 - core) * LANES, LANES)
        mine[k] = low[:, pl.ds(at, LANES)]
        theirs[k] = bf(low[:, pl.ds(to, LANES)])
    at = pl.multiple_of((z * TP_COUNT + core) * LANES, LANES)
    new, old = iota((count, rows), 0), iota((count, rows), 1)
    pick = hot(old == div(new, seqs) * (Y_COUNT * seqs) + y * seqs + rem(new, seqs))
    slab[...] = matmul(pick, xt[pl.ds(at, LANES), :], NT)


def load_mix(a0, a1, a2, a3, w_mix, sems):
    _, y, _ = place()
    moves = []
    for k, part in enumerate((a0, a1, a2, a3)):
        to = rem(y - k + Y_COUNT, Y_COUNT)
        moves.append(
            pltpu.make_async_copy(
                part.at[pl.ds(LANES, w_mix.shape[1])], w_mix.at[to], sems.at[k]
            )
        )
    for move in moves:
        move.start()
    for move in moves:
        move.wait()


def load_parts(*refs):
    *parts, held, sems = refs
    moves = [
        pltpu.make_async_copy(part.at[pl.ds(0, held.shape[1])], held.at[k], sems.at[k])
        for k, part in enumerate(parts)
    ]
    for move in moves:
        move.start()
    for move in moves:
        move.wait()


def pack_early(query, forget, inputs, out_gate, mix, packed, out, *scratch):
    *held, sems = scratch
    moves = [
        pltpu.make_async_copy(w, held[k], sems.at[k])
        for k, w in enumerate((query, forget, inputs, out_gate))
    ]
    rest = out.shape[0] - LANES
    moves.append(pltpu.make_async_copy(mix, out.at[pl.ds(LANES, rest)], sems.at[4]))
    for move in moves:
        move.start()
    heads, per, _ = query.shape
    for k in range(4):
        moves[k].wait()
        for h in range(0, heads, 4):
            block = jnp.concatenate([f32(held[k][h + n]) for n in range(4)], axis=0)
            at = (k * heads + h) * per
            out[at : at + 4 * per, :] = bf(block)
    moves[4].wait()
    move = pltpu.make_async_copy(out, packed, sems.at[5])
    move.start()
    move.wait()


def flipped(x, out):
    out[...] = x[...].T


def assemble(tiles, rows):
    count = tiles.shape[0]
    for k in range(count):
        rows[:, k * LANES : (k + 1) * LANES] = tiles[k]


def normed_of(rows, gain):
    values = f32(rows[...])
    scale = lax.rsqrt(jnp.mean(values * values, axis=1, keepdims=True) + EPS)
    return bf(values * scale * gain[...])


def projections(tiles, gain, w_held, a3, channels, residual, rows, weights, sems):
    z, y, core = place()
    last = pltpu.make_async_copy(a3.at[pl.ds(0, LANES)], weights, sems.at[0])
    last.start()
    assemble(tiles, rows)
    normed = normed_of(rows, gain)
    flats = []
    for k in range(Y_COUNT - 1):
        flats.append(bf(matmul(normed, w_held[k], NT)))
    last.wait()
    flats.append(bf(matmul(normed, weights[...], NT)))
    count = rows.shape[0]
    seqs = count // Z_COUNT
    stacked = jnp.concatenate(flats, axis=0)
    shape = (Z_COUNT * 16, Y_COUNT * count)
    new, old = iota(shape, 0), iota(shape, 1)
    row = div(new, 16) * seqs + div(rem(new, 16), Y_COUNT)
    wanted = rem(y - rem(new, Y_COUNT) + Y_COUNT, Y_COUNT) * count + row
    real = div(rem(new, 16), Y_COUNT) < seqs
    channels[...] = bf(matmul(hot((old == wanted) & real), stacked, NN))
    at = pl.multiple_of(z * TP_COUNT * LANES, 2 * LANES)
    both = rows[:, pl.ds(at, TP_COUNT * LANES)]
    shape = (TP_COUNT * LANES, LANES)
    old, new = iota(shape, 0), iota(shape, 1)
    each = LANES // Y_COUNT
    wanted = div(new, each) * (TP_COUNT * each) + core * each + rem(new, each)
    residual[...] = matmul(both, hot(old == wanted), NN)


def channel_views(arrived, k):
    per = LANES // KV_COUNT
    shape = (LANES, Z_COUNT * 16)
    channel, source = iota(shape, 0), iota(shape, 1)
    kv = div(channel, per)
    wanted = div(kv, Y_COUNT) * 16 + k * Y_COUNT + rem(kv, Y_COUNT)
    wide = matmul(hot(source == wanted), arrived, NN)
    shape = (LANES, LANES)
    own = rem(iota(shape, 0), per) == rem(iota(shape, 1), per)
    wide = bf(jnp.where(own, wide, 0.0))
    shape = (LANES, KV_COUNT)
    gather = hot(div(iota(shape, 0), per) == iota(shape, 1))
    shape = (KV_COUNT, LANES)
    gather_rows = hot(div(iota(shape, 1), per) == iota(shape, 0))
    return matmul(wide, gather, NN), matmul(gather_rows, wide, NT)


def read_state(arrived, floor_rows, floor_t, gain, state, merged, vectors):
    seqs, heads = state.shape[:2]
    floor = floor_t[...]
    for k in range(seqs):
        columns, lines = channel_views(arrived[...], k)
        query = columns[:, :heads]
        raw = columns[:, heads : 2 * heads]
        forget = floor + (1.0 - floor) * jax.nn.sigmoid(raw)
        keep = (1.0 - floor) * jax.nn.sigmoid(-raw)
        line = lines[2 * heads : 3 * heads]
        raw = lines[heads : 2 * heads]
        low = floor_rows[...]
        vectors[k, :heads] = low + (1.0 - low) * jax.nn.sigmoid(raw)
        vectors[k, heads : 2 * heads] = (1.0 - low) * jax.nn.sigmoid(-raw)
        vectors[k, 2 * heads :] = line
        weight = query * forget
        added = jnp.sum(query * keep, axis=0, keepdims=True)
        outs = []
        for h in range(heads):
            term = weight[:, h : h + 1] * state[k, h]
            outs.append(
                jnp.sum(term, axis=0, keepdims=True) + added[:, h : h + 1] * line[h : h + 1]
            )
        readout = jnp.concatenate(outs, axis=0)
        scale = lax.rsqrt(jnp.mean(readout * readout, axis=1, keepdims=True) + EPS)
        gated = readout * scale * gain[...] * jax.nn.silu(lines[3 * heads : 4 * heads])
        merged[k * heads : (k + 1) * heads, :] = gated


def next_state(state, vectors, out, held, sems):
    seqs, heads = state.shape[:2]
    moves = []
    for k in range(seqs):
        columns = vectors[k].T
        for h in range(heads):
            line = vectors[k, 2 * heads + h : 2 * heads + h + 1, :]
            held[k, h] = (
                columns[:, h : h + 1] * state[k, h] + columns[:, heads + h : heads + h + 1] * line
            )
        move = pltpu.make_async_copy(held.at[k], out.at[k], sems.at[k])
        move.start()
        moves.append(move)
    for move in moves:
        move.wait()


def mix_out(tiles, w_mix, residual, after, rows):
    _, heads_rows, _ = tiles.shape
    slab_rows = rows.shape[0]
    seqs = slab_rows // Z_COUNT
    heads = heads_rows // seqs
    total = Z_COUNT * heads_rows
    shape = (total, total)
    new, old = iota(shape, 0), iota(shape, 1)
    row = rem(new, slab_rows)
    wanted = (
        div(row, seqs) * heads_rows + rem(row, seqs) * heads + div(new, slab_rows)
    )
    order = hot(old == wanted)
    for t in range(TP_COUNT):
        stacked = jnp.concatenate([tiles[z * TP_COUNT + t] for z in range(Z_COUNT)], axis=0)
        moved = bf(matmul(order, stacked, NN))
        for h in range(heads):
            at = (t * heads + h) * LANES
            rows[:, at : at + LANES] = moved[h * slab_rows : (h + 1) * slab_rows]
    weights = w_mix[...].reshape(LANES, rows.shape[1])
    after[...] = bf(residual[...] + matmul(rows[...], weights, NT))


def lane_order(transposed):
    shape = (TP_COUNT * LANES, TP_COUNT * LANES)
    each = LANES // Y_COUNT
    a, b = (0, 1) if not transposed else (1, 0)
    old, new = iota(shape, a), iota(shape, b)
    wanted = (
        rem(div(new, each), TP_COUNT) * LANES
        + div(new, TP_COUNT * each) * each
        + rem(new, each)
    )
    return hot(old == wanted)


def second_block(
    tiles, gain, after, w_held, t3, d0, d1, d2, d3, out, rows, w_last, w_down, sems
):
    z, _, core = place()
    moves = [
        pltpu.make_async_copy(part, w_down.at[k], sems.at[k])
        for k, part in enumerate((d0, d1, d2, d3))
    ]
    last = pltpu.make_async_copy(t3, w_last, sems.at[Y_COUNT])
    last.start()
    for move in moves:
        move.start()
    order = lane_order(False)
    wide = TP_COUNT * LANES
    count = rows.shape[0]
    pairs = [
        jnp.concatenate([tiles[k * TP_COUNT], tiles[k * TP_COUNT + 1]], axis=1)
        for k in range(Z_COUNT)
    ]
    ordered = bf(matmul(jnp.concatenate(pairs, axis=0), order, NN))
    for k in range(Z_COUNT):
        rows[:, k * wide : (k + 1) * wide] = ordered[k * count : (k + 1) * count]
    normed = normed_of(rows, gain)
    hidden = w_down.shape[1]
    mids = []
    for k in range(Y_COUNT):
        if k == Y_COUNT - 1:
            last.wait()
            w_top = w_last[...]
        else:
            w_top = w_held[k]
        tops = matmul(normed, w_top, NT)
        mids.append(bf(jax.nn.silu(tops[:, :hidden]) * tops[:, hidden:]))
    total = jnp.zeros(rows.shape, jnp.float32)
    for k, move in enumerate(moves):
        move.wait()
        total += matmul(mids[k], w_down[k], NN)
    each = LANES // Y_COUNT
    total = 0.5 * total
    spare = jnp.zeros((each - count, LANES), jnp.float32)

    def spread(block):
        padded = jnp.concatenate([block, spare], axis=0)
        return jnp.concatenate([padded] * Y_COUNT, axis=0).T

    group = div(iota((8, LANES), 1), each)
    home = spread(f32(after[...]))
    for k in range(Z_COUNT * TP_COUNT):
        block = spread(total[:, k * LANES : (k + 1) * LANES])
        for n in range(Y_COUNT):
            where = rem(k, TP_COUNT) * Y_COUNT + n
            own_y, t = div(where, TP_COUNT), rem(where, TP_COUNT)
            packed = jnp.zeros((8, LANES), jnp.float32)
            extra = jnp.zeros((8, LANES), jnp.float32)
            for g in range(Y_COUNT):
                at, to = n * each + g * 8, own_y * each + g * 8
                packed = jnp.where(group == g, block[at : at + 8], packed)
                extra = jnp.where(group == g, home[to : to + 8], extra)
            own = (z == div(k, TP_COUNT)) & (core == t)
            packed = packed + jnp.where(own, extra, 0.0)
            out[(div(k, TP_COUNT) * Y_COUNT + own_y) * TP_COUNT + t] = bf(packed)


def finish(arrived, out):
    cols, rows = out.shape
    slab_rows = rows // Y_COUNT
    seqs = slab_rows // Z_COUNT
    lanes_each = LANES // Y_COUNT
    parts = []
    for k in range(Y_COUNT):
        part = jnp.zeros(arrived.shape[1:], jnp.float32)
        for n in range(Z_COUNT):
            for t in range(TP_COUNT):
                part += f32(arrived[(n * Y_COUNT + k) * TP_COUNT + t])
        parts.append(bf(part))
    sums = jnp.concatenate(parts, axis=1)
    shape = (Y_COUNT * LANES, rows)
    old, new = iota(shape, 0), iota(shape, 1)
    y = rem(div(new, seqs), Y_COUNT)
    row = div(new, seqs * Y_COUNT) * seqs + rem(new, seqs)
    for g in range(cols // 8):
        pick = hot(old == y * LANES + g * lanes_each + row)
        out[g * 8 : (g + 1) * 8, :] = bf(matmul(sums, pick, NN))


def shards(
    hidden_in,
    state,
    forget_floor,
    ffn_gain_one,
    w_gate_one,
    w_up_one,
    w_down_one,
    mix_gain,
    w_query,
    w_forget,
    w_input,
    w_outgate,
    head_gain,
    w_mix_out,
    ffn_gain_two,
    w_gate_two,
    w_up_two,
    w_down_two,
):
    rows, own_cols = hidden_in.shape
    width, hidden = w_gate_one.shape
    seqs, heads = state.shape[:2]
    slab_rows = rows // Y_COUNT
    half16, half32 = jnp.bfloat16, jnp.float32
    dma = pltpu.SemaphoreType.DMA

    kinds = [jnp.transpose(w, (1, 2, 0)) for w in (w_query, w_forget, w_input, w_outgate)]
    (early,) = local(
        pack_early,
        [((LANES + own_cols, width), half16)],
        *kinds,
        w_mix_out.T,
        scratch=(
            pltpu.VMEM((LANES + own_cols, width), half16),
            *[pltpu.VMEM(k.shape, half16) for k in kinds],
            dma((6,)),
        ),
        outside=(0, 1, 2, 3, 4),
        held_out=True,
        sent=(0,),
    )
    late_top = jnp.concatenate([w_gate_two.T, w_up_two.T], axis=0)

    (floor_t,) = local(flipped, [((LANES, heads), half32)], forget_floor)

    own = exchange(copies(hidden_in.T, KV_COUNT), "kv")
    first_w = local(
        load_first,
        [((hidden, width), half16)] * 3,
        w_gate_one.T,
        w_up_one.T,
        w_down_one,
        scratch=(dma((3,)),),
        outside=(0, 1, 2),
        held_out=True,
        vmem=True,
    )
    other = swap_cores(own)
    mine, theirs, slab = local(
        first_block,
        [
            ((Z_COUNT, rows, LANES), half32),
            ((Z_COUNT, rows, LANES), half16),
            ((slab_rows, LANES), half32),
        ],
        own,
        other,
        ffn_gain_one.reshape(-1, LANES),
        *first_w,
        scratch=(pltpu.VMEM((width, rows), half16), pltpu.VMEM((rows, width), half32)),
    )
    both = bf(mine + f32(swap_cores(theirs)))
    summed = exchange(both.reshape(KV_COUNT, slab_rows, LANES), "kv")
    below, above = shift_y(early, 1), shift_y(early, -1)
    twice = shift_y(below, 1)
    after_own = bf(slab + 0.5 * f32(summed).sum(axis=0))

    top_above = shift_y(late_top, -1)
    top_below = shift_y(late_top, 1)
    low_above = shift_y(w_down_two, -1)
    low_below = shift_y(w_down_two, 1)
    top_far = shift_y(top_above, -1)
    low_far = shift_y(low_above, -1)
    tops = (late_top, top_below, top_above, top_far)
    lows = (w_down_two, low_below, low_above, low_far)

    after_tiles = slab_exchange(after_own)
    parts = (early, below, twice, above)
    (w_held,) = local(
        load_parts,
        [((Y_COUNT - 1, LANES, width), half16)],
        *parts[:-1],
        scratch=(dma((Y_COUNT - 1,)),),
        outside=(0, 1, 2),
        held_out=True,
        vmem=True,
    )
    channels, residual = local(
        projections,
        [((Z_COUNT * 16, LANES), half16), ((slab_rows, LANES), half32)],
        after_tiles,
        mix_gain.reshape(1, -1),
        w_held,
        parts[-1],
        scratch=(
            pltpu.VMEM((slab_rows, width), half16),
            pltpu.VMEM((LANES, width), half16),
            dma((1,)),
        ),
        outside=(3,),
        held_out=True,
    )
    zgroups = [[a * Y_COUNT + b for a in range(Z_COUNT)] for b in range(Y_COUNT)]
    arrived = exchange(channels.reshape(Z_COUNT, 16, LANES), "kv", zgroups)
    held = state
    gated, vectors = local(
        read_state,
        [((seqs * heads, LANES), half32), ((seqs, 3 * heads, LANES), half32)],
        arrived.reshape(Z_COUNT * 16, LANES),
        forget_floor,
        floor_t,
        head_gain,
        held,
    )
    merged_tiles = slab_exchange(bf(gated))
    (new_state,) = local(
        next_state,
        [(state.shape, half32)],
        held,
        vectors,
        scratch=(pltpu.VMEM(state.shape, half32), dma((seqs,))),
        sent=(0,),
    )
    (w_mix,) = local(
        load_mix,
        [((Y_COUNT, own_cols, width), half16)],
        *parts,
        scratch=(dma((Y_COUNT,)),),
        outside=(0, 1, 2, 3),
        held_out=True,
        vmem=True,
    )
    (after_mix,) = local(
        mix_out,
        [((slab_rows, LANES), half16)],
        merged_tiles,
        w_mix,
        residual,
        scratch=(pltpu.VMEM((slab_rows, width), half16),),
    )

    mix_tiles = slab_exchange(after_mix)
    (w_held,) = local(
        load_parts,
        [((Y_COUNT - 1, 2 * hidden, width), half16)],
        *tops[:-1],
        scratch=(dma((Y_COUNT - 1,)),),
        outside=(0, 1, 2),
        vmem=True,
    )
    (messages,) = local(
        second_block,
        [((KV_COUNT * TP_COUNT, 8, LANES), half16)],
        mix_tiles,
        ffn_gain_two.reshape(1, -1),
        after_mix,
        w_held,
        tops[-1],
        *lows,
        scratch=(
            pltpu.VMEM((slab_rows, width), half16),
            pltpu.VMEM((2 * hidden, width), half16),
            pltpu.VMEM((Y_COUNT, hidden, width), half16),
            dma((Y_COUNT + 1,)),
        ),
        outside=(4, 5, 6, 7, 8),
    )
    arrived = exchange(messages, ("kv", "tp"))
    (result,) = local(finish, [((own_cols, rows), half16)], arrived)
    return (result.T, new_state)


def solution(mesh):
    return jax.shard_map(
        shards,
        mesh=mesh,
        in_specs=(
            P("dp", ("kv", "tp")),
            P(("dp", "kv"), "tp", None, None),
            P("tp", None),
            P(),
            P(None, ("kv", "tp")),
            P(None, ("kv", "tp")),
            P(("kv", "tp"), None),
            P(),
            P(None, "tp", "kv"),
            P(None, "tp", "kv"),
            P(None, "tp", "kv"),
            P(None, "tp", "kv"),
            P("tp", None),
            P(None, ("kv", "tp")),
            P(),
            P(None, ("kv", "tp")),
            P(None, ("kv", "tp")),
            P(("kv", "tp"), None),
        ),
        out_specs=(P("dp", ("kv", "tp")), P(("dp", "kv"), "tp", None, None)),
        check_vma=False,
    )
```

```python
import jax
import jax.numpy as jnp
from jax import lax
from jax.experimental import pallas as pl
from jax.experimental.pallas import tpu as pltpu
from jax.sharding import PartitionSpec as P

EPS = 1e-06
LANES = 128
Z_COUNT, Y_COUNT, TP_COUNT = 8, 4, 2
KV_COUNT = Z_COUNT * Y_COUNT
NN, NT = ((1,), (0,)), ((1,), (1,))


def bf(x):
    return x.astype(jnp.bfloat16)


def f32(x):
    return x.astype(jnp.float32)


def matmul(a, b, dims):
    return lax.dot_general(a, b, (dims, ((), ())), preferred_element_type=jnp.float32)


def exchange(tiles, axis, groups=None):
    return lax.all_to_all(
        tiles, axis, split_axis=0, concat_axis=0, axis_index_groups=groups, tiled=True
    )


def copies(x, count):
    return jnp.broadcast_to(x, (count, *x.shape))


def swap_cores(x):
    return lax.ppermute(x, "tp", [(0, 1), (1, 0)])


def shift_y(x, step):
    pairs = [
        (z * Y_COUNT + y, z * Y_COUNT + (y + step) % Y_COUNT)
        for z in range(Z_COUNT)
        for y in range(Y_COUNT)
    ]
    return lax.ppermute(x, "kv", pairs)


def slab_exchange(x):
    groups = [
        [(z * Y_COUNT + y) * TP_COUNT + t for z in range(Z_COUNT) for t in range(TP_COUNT)]
        for y in range(Y_COUNT)
    ]
    return exchange(copies(x, Z_COUNT * TP_COUNT), ("kv", "tp"), groups)


def div(v, d):
    if d & (d - 1) == 0:
        return v >> (d.bit_length() - 1)
    return (v * (65536 // d + 1)) >> 16


def rem(v, d):
    return v & (d - 1) if d & (d - 1) == 0 else v - div(v, d) * d


def place():
    kv = lax.axis_index("kv")
    return div(kv, Y_COUNT), rem(kv, Y_COUNT), lax.axis_index("tp")


def iota(shape, axis):
    return lax.broadcasted_iota(jnp.int32, shape, axis)


def hot(mask):
    return jnp.where(mask, 1.0, 0.0).astype(jnp.bfloat16)


def local(body, outs, *args, scratch=(), outside=(), held_out=False, vmem=False, sent=(), flops=1 << 20):
    kind = pltpu.VMEM if vmem else jax.ShapeDtypeStruct
    shapes = [pltpu.HBM(s, d) if k in sent else kind(s, d) for k, (s, d) in enumerate(outs)]
    placed = [
        pl.BlockSpec(memory_space=pltpu.HBM) if k in sent else pl.BlockSpec(memory_space=pltpu.VMEM)
        for k in range(len(outs))
    ]
    held = pl.BlockSpec(memory_space=pltpu.VMEM)
    specs = [pl.BlockSpec(memory_space=pl.ANY) if k in outside else held for k in range(len(args))]
    args = [
        pltpu.with_memory_space_constraint(a, pltpu.HBM) if held_out and k in outside else a
        for k, a in enumerate(args)
    ]
    size = sum(a.size * a.dtype.itemsize for a in args)
    return pl.pallas_call(
        body,
        out_shape=shapes,
        in_specs=specs,
        out_specs=placed,
        scratch_shapes=list(scratch),
        compiler_params=pltpu.CompilerParams(vmem_limit_bytes=VMEM_LIMIT),
        cost_estimate=pl.CostEstimate(flops=flops, bytes_accessed=size, transcendentals=0),
    )(*args)


VMEM_LIMIT = 24 * 1024 * 1024


def load_first(w_gate, w_up, w_down, gate, upper, down, sems):
    moves = [
        pltpu.make_async_copy(src, dst, sems.at[k])
        for k, (src, dst) in enumerate(((w_gate, gate), (w_up, upper), (w_down, down)))
    ]
    for move in moves:
        move.start()
    for move in moves:
        move.wait()


def first_block(own, other, gain, w_gate, w_up, w_down, theirs, slab, mid_out, xt):
    z, y, core = place()
    cols = own.shape[1]
    for kv in range(KV_COUNT):
        base = kv * TP_COUNT * cols
        xt[pl.ds(pl.multiple_of(base + core * cols, cols), cols), :] = own[kv]
        xt[pl.ds(pl.multiple_of(base + (1 - core) * cols, cols), cols), :] = other[kv]
    width, rows = xt.shape
    square = jnp.zeros((8, rows), jnp.float32)
    for c in range(width // LANES):
        part = f32(xt[c * LANES : (c + 1) * LANES, :])
        square += (part * part).reshape(LANES // 8, 8, rows).sum(axis=0)
    scale = lax.rsqrt(square.sum(axis=0, keepdims=True) * (1.0 / width) + EPS)
    gains = gain[...].T
    normed = []
    for c in range(width // LANES):
        part = f32(xt[c * LANES : (c + 1) * LANES, :])
        normed.append(bf(part * scale * gains[:, c : c + 1]))
    normed = jnp.concatenate(normed, axis=0)
    gate = matmul(w_gate[...], normed, NN)
    upper = matmul(w_up[...], normed, NN)
    mid = bf(jax.nn.silu(gate) * upper)
    count = slab.shape[0]
    seqs = count // Z_COUNT
    new, old = iota((rows, rows), 0), iota((rows, rows), 1)
    wanted = (
        div(rem(new, count), seqs) * (Y_COUNT * seqs)
        + div(new, count) * seqs
        + rem(new, seqs)
    )
    mid = bf(matmul(hot(old == wanted), mid, NT))
    mid_out[...] = mid
    for k in range(Z_COUNT):
        to = pl.multiple_of((k * TP_COUNT + 1 - core) * LANES, LANES)
        theirs[k] = bf(matmul(mid, w_down[:, pl.ds(to, LANES)], NN))
    at = pl.multiple_of((z * TP_COUNT + core) * LANES, LANES)
    new, old = iota((count, rows), 0), iota((count, rows), 1)
    pick = hot(old == div(new, seqs) * (Y_COUNT * seqs) + y * seqs + rem(new, seqs))
    slab[...] = matmul(pick, xt[pl.ds(at, LANES), :], NT)


def own_half(mid, w_down, mine):
    _, _, core = place()
    for k in range(Z_COUNT):
        at = pl.multiple_of((k * TP_COUNT + core) * LANES, LANES)
        mine[k] = matmul(mid[...], w_down[:, pl.ds(at, LANES)], NN)


def load_mix(a0, a1, a2, a3, w_mix, sems):
    _, y, _ = place()
    moves = []
    for k, part in enumerate((a0, a1, a2, a3)):
        to = rem(y - k + Y_COUNT, Y_COUNT)
        moves.append(
            pltpu.make_async_copy(
                part.at[pl.ds(LANES, w_mix.shape[1])], w_mix.at[to], sems.at[k]
            )
        )
    for move in moves:
        move.start()
    for move in moves:
        move.wait()


def load_parts(*refs):
    *parts, held, sems = refs
    moves = [
        pltpu.make_async_copy(part.at[pl.ds(0, held.shape[1])], held.at[k], sems.at[k])
        for k, part in enumerate(parts)
    ]
    for move in moves:
        move.start()
    for move in moves:
        move.wait()


def pack_early(query, forget, inputs, out_gate, mix, packed, out, *scratch):
    *held, sems = scratch
    moves = [
        pltpu.make_async_copy(w, held[k], sems.at[k])
        for k, w in enumerate((query, forget, inputs, out_gate))
    ]
    rest = out.shape[0] - LANES
    moves.append(pltpu.make_async_copy(mix, out.at[pl.ds(LANES, rest)], sems.at[4]))
    for move in moves:
        move.start()
    heads, per, _ = query.shape
    for k in range(4):
        moves[k].wait()
        for h in range(0, heads, 4):
            block = jnp.concatenate([f32(held[k][h + n]) for n in range(4)], axis=0)
            at = (k * heads + h) * per
            out[at : at + 4 * per, :] = bf(block)
    moves[4].wait()
    move = pltpu.make_async_copy(out, packed, sems.at[5])
    move.start()
    move.wait()


def flipped(x, out):
    out[...] = x[...].T


def assemble(tiles, rows):
    count = tiles.shape[0]
    for k in range(count):
        rows[:, k * LANES : (k + 1) * LANES] = tiles[k]


def normed_of(rows, gain):
    values = f32(rows[...])
    scale = lax.rsqrt(jnp.mean(values * values, axis=1, keepdims=True) + EPS)
    return bf(values * scale * gain[...])


def projections(tiles, gain, w_held, a3, channels, residual, rows, weights, sems):
    z, y, core = place()
    last = pltpu.make_async_copy(a3.at[pl.ds(0, LANES)], weights, sems.at[0])
    last.start()
    assemble(tiles, rows)
    normed = normed_of(rows, gain)
    flats = []
    for k in range(Y_COUNT - 1):
        flats.append(bf(matmul(normed, w_held[k], NT)))
    last.wait()
    flats.append(bf(matmul(normed, weights[...], NT)))
    count = rows.shape[0]
    seqs = count // Z_COUNT
    stacked = jnp.concatenate(flats, axis=0)
    shape = (Z_COUNT * 16, Y_COUNT * count)
    new, old = iota(shape, 0), iota(shape, 1)
    row = div(new, 16) * seqs + div(rem(new, 16), Y_COUNT)
    wanted = rem(y - rem(new, Y_COUNT) + Y_COUNT, Y_COUNT) * count + row
    real = div(rem(new, 16), Y_COUNT) < seqs
    channels[...] = bf(matmul(hot((old == wanted) & real), stacked, NN))
    at = pl.multiple_of(z * TP_COUNT * LANES, 2 * LANES)
    both = rows[:, pl.ds(at, TP_COUNT * LANES)]
    shape = (TP_COUNT * LANES, LANES)
    old, new = iota(shape, 0), iota(shape, 1)
    each = LANES // Y_COUNT
    wanted = div(new, each) * (TP_COUNT * each) + core * each + rem(new, each)
    residual[...] = matmul(both, hot(old == wanted), NN)


def channel_views(arrived, k):
    per = LANES // KV_COUNT
    shape = (LANES, Z_COUNT * 16)
    channel, source = iota(shape, 0), iota(shape, 1)
    kv = div(channel, per)
    wanted = div(kv, Y_COUNT) * 16 + k * Y_COUNT + rem(kv, Y_COUNT)
    wide = matmul(hot(source == wanted), arrived, NN)
    shape = (LANES, LANES)
    own = rem(iota(shape, 0), per) == rem(iota(shape, 1), per)
    wide = bf(jnp.where(own, wide, 0.0))
    shape = (LANES, KV_COUNT)
    gather = hot(div(iota(shape, 0), per) == iota(shape, 1))
    shape = (KV_COUNT, LANES)
    gather_rows = hot(div(iota(shape, 1), per) == iota(shape, 0))
    return matmul(wide, gather, NN), matmul(gather_rows, wide, NT)


def read_state(arrived, floor_rows, floor_t, gain, state, merged, vectors):
    seqs, heads = state.shape[:2]
    floor = floor_t[...]
    for k in range(seqs):
        columns, lines = channel_views(arrived[...], k)
        query = columns[:, :heads]
        raw = columns[:, heads : 2 * heads]
        forget = floor + (1.0 - floor) * jax.nn.sigmoid(raw)
        keep = (1.0 - floor) * jax.nn.sigmoid(-raw)
        line = lines[2 * heads : 3 * heads]
        raw = lines[heads : 2 * heads]
        low = floor_rows[...]
        vectors[k, :heads] = low + (1.0 - low) * jax.nn.sigmoid(raw)
        vectors[k, heads : 2 * heads] = (1.0 - low) * jax.nn.sigmoid(-raw)
        vectors[k, 2 * heads :] = line
        weight = query * forget
        added = jnp.sum(query * keep, axis=0, keepdims=True)
        outs = []
        for h in range(heads):
            term = weight[:, h : h + 1] * state[k, h]
            outs.append(
                jnp.sum(term, axis=0, keepdims=True) + added[:, h : h + 1] * line[h : h + 1]
            )
        readout = jnp.concatenate(outs, axis=0)
        scale = lax.rsqrt(jnp.mean(readout * readout, axis=1, keepdims=True) + EPS)
        gated = readout * scale * gain[...] * jax.nn.silu(lines[3 * heads : 4 * heads])
        merged[k * heads : (k + 1) * heads, :] = gated


def next_state(state, vectors, out, held, sems):
    seqs, heads = state.shape[:2]
    moves = []
    for k in range(seqs):
        columns = vectors[k].T
        for h in range(heads):
            line = vectors[k, 2 * heads + h : 2 * heads + h + 1, :]
            held[k, h] = (
                columns[:, h : h + 1] * state[k, h] + columns[:, heads + h : heads + h + 1] * line
            )
        move = pltpu.make_async_copy(held.at[k], out.at[k], sems.at[k])
        move.start()
        moves.append(move)
    for move in moves:
        move.wait()


def mix_out(tiles, w_mix, residual, after, rows):
    _, heads_rows, _ = tiles.shape
    slab_rows = rows.shape[0]
    seqs = slab_rows // Z_COUNT
    heads = heads_rows // seqs
    total = Z_COUNT * heads_rows
    shape = (total, total)
    new, old = iota(shape, 0), iota(shape, 1)
    row = rem(new, slab_rows)
    wanted = (
        div(row, seqs) * heads_rows + rem(row, seqs) * heads + div(new, slab_rows)
    )
    order = hot(old == wanted)
    for t in range(TP_COUNT):
        stacked = jnp.concatenate([tiles[z * TP_COUNT + t] for z in range(Z_COUNT)], axis=0)
        moved = bf(matmul(order, stacked, NN))
        for h in range(heads):
            at = (t * heads + h) * LANES
            rows[:, at : at + LANES] = moved[h * slab_rows : (h + 1) * slab_rows]
    weights = w_mix[...].reshape(LANES, rows.shape[1])
    after[...] = bf(residual[...] + matmul(rows[...], weights, NT))


def lane_order(transposed):
    shape = (TP_COUNT * LANES, TP_COUNT * LANES)
    each = LANES // Y_COUNT
    a, b = (0, 1) if not transposed else (1, 0)
    old, new = iota(shape, a), iota(shape, b)
    wanted = (
        rem(div(new, each), TP_COUNT) * LANES
        + div(new, TP_COUNT * each) * each
        + rem(new, each)
    )
    return hot(old == wanted)


def second_block(
    tiles, gain, after, w_held, t3, d0, d1, d2, d3, out, rows, w_last, w_down, sems
):
    z, _, core = place()
    moves = [
        pltpu.make_async_copy(part, w_down.at[k], sems.at[k])
        for k, part in enumerate((d0, d1, d2, d3))
    ]
    last = pltpu.make_async_copy(t3, w_last, sems.at[Y_COUNT])
    last.start()
    for move in moves:
        move.start()
    order = lane_order(False)
    wide = TP_COUNT * LANES
    count = rows.shape[0]
    pairs = [
        jnp.concatenate([tiles[k * TP_COUNT], tiles[k * TP_COUNT + 1]], axis=1)
        for k in range(Z_COUNT)
    ]
    ordered = bf(matmul(jnp.concatenate(pairs, axis=0), order, NN))
    for k in range(Z_COUNT):
        rows[:, k * wide : (k + 1) * wide] = ordered[k * count : (k + 1) * count]
    normed = normed_of(rows, gain)
    hidden = w_down.shape[1]
    mids = []
    for k in range(Y_COUNT):
        if k == Y_COUNT - 1:
            last.wait()
            w_top = w_last[...]
        else:
            w_top = w_held[k]
        tops = matmul(normed, w_top, NT)
        mids.append(bf(jax.nn.silu(tops[:, :hidden]) * tops[:, hidden:]))
    total = jnp.zeros(rows.shape, jnp.float32)
    for k, move in enumerate(moves):
        move.wait()
        total += matmul(mids[k], w_down[k], NN)
    each = LANES // Y_COUNT
    total = 0.5 * total
    spare = jnp.zeros((each - count, LANES), jnp.float32)

    def spread(block):
        padded = jnp.concatenate([block, spare], axis=0)
        return jnp.concatenate([padded] * Y_COUNT, axis=0).T

    group = div(iota((8, LANES), 1), each)
    home = spread(f32(after[...]))
    for k in range(Z_COUNT * TP_COUNT):
        block = spread(total[:, k * LANES : (k + 1) * LANES])
        for n in range(Y_COUNT):
            where = rem(k, TP_COUNT) * Y_COUNT + n
            own_y, t = div(where, TP_COUNT), rem(where, TP_COUNT)
            packed = jnp.zeros((8, LANES), jnp.float32)
            extra = jnp.zeros((8, LANES), jnp.float32)
            for g in range(Y_COUNT):
                at, to = n * each + g * 8, own_y * each + g * 8
                packed = jnp.where(group == g, block[at : at + 8], packed)
                extra = jnp.where(group == g, home[to : to + 8], extra)
            own = (z == div(k, TP_COUNT)) & (core == t)
            packed = packed + jnp.where(own, extra, 0.0)
            out[(div(k, TP_COUNT) * Y_COUNT + own_y) * TP_COUNT + t] = bf(packed)


def finish(arrived, out):
    cols, rows = out.shape
    slab_rows = rows // Y_COUNT
    seqs = slab_rows // Z_COUNT
    lanes_each = LANES // Y_COUNT
    parts = []
    for k in range(Y_COUNT):
        part = jnp.zeros(arrived.shape[1:], jnp.float32)
        for n in range(Z_COUNT):
            for t in range(TP_COUNT):
                part += f32(arrived[(n * Y_COUNT + k) * TP_COUNT + t])
        parts.append(bf(part))
    sums = jnp.concatenate(parts, axis=1)
    shape = (Y_COUNT * LANES, rows)
    old, new = iota(shape, 0), iota(shape, 1)
    y = rem(div(new, seqs), Y_COUNT)
    row = div(new, seqs * Y_COUNT) * seqs + rem(new, seqs)
    for g in range(cols // 8):
        pick = hot(old == y * LANES + g * lanes_each + row)
        out[g * 8 : (g + 1) * 8, :] = bf(matmul(sums, pick, NN))


def shards(
    hidden_in,
    state,
    forget_floor,
    ffn_gain_one,
    w_gate_one,
    w_up_one,
    w_down_one,
    mix_gain,
    w_query,
    w_forget,
    w_input,
    w_outgate,
    head_gain,
    w_mix_out,
    ffn_gain_two,
    w_gate_two,
    w_up_two,
    w_down_two,
):
    rows, own_cols = hidden_in.shape
    width, hidden = w_gate_one.shape
    seqs, heads = state.shape[:2]
    slab_rows = rows // Y_COUNT
    half16, half32 = jnp.bfloat16, jnp.float32
    dma = pltpu.SemaphoreType.DMA

    kinds = [jnp.transpose(w, (1, 2, 0)) for w in (w_query, w_forget, w_input, w_outgate)]
    (early,) = local(
        pack_early,
        [((LANES + own_cols, width), half16)],
        *kinds,
        w_mix_out.T,
        scratch=(
            pltpu.VMEM((LANES + own_cols, width), half16),
            *[pltpu.VMEM(k.shape, half16) for k in kinds],
            dma((6,)),
        ),
        outside=(0, 1, 2, 3, 4),
        held_out=True,
        sent=(0,),
    )
    late_top = jnp.concatenate([w_gate_two.T, w_up_two.T], axis=0)

    (floor_t,) = local(flipped, [((LANES, heads), half32)], forget_floor)

    own = exchange(copies(hidden_in.T, KV_COUNT), "kv")
    first_w = local(
        load_first,
        [((hidden, width), half16)] * 3,
        w_gate_one.T,
        w_up_one.T,
        w_down_one,
        scratch=(dma((3,)),),
        outside=(0, 1, 2),
        held_out=True,
        vmem=True,
    )
    other = swap_cores(own)
    theirs, slab, mid = local(
        first_block,
        [
            ((Z_COUNT, rows, LANES), half16),
            ((slab_rows, LANES), half32),
            ((rows, hidden), half16),
        ],
        own,
        other,
        ffn_gain_one.reshape(-1, LANES),
        *first_w,
        scratch=(pltpu.VMEM((width, rows), half16),),
    )
    from_other = swap_cores(theirs)
    (mine,) = local(own_half, [((Z_COUNT, rows, LANES), half32)], mid, first_w[2])
    both = bf(mine + f32(from_other))
    summed = exchange(both.reshape(KV_COUNT, slab_rows, LANES), "kv")
    below, above = shift_y(early, 1), shift_y(early, -1)
    twice = shift_y(below, 1)
    after_own = bf(slab + 0.5 * f32(summed).sum(axis=0))

    top_above = shift_y(late_top, -1)
    top_below = shift_y(late_top, 1)
    low_above = shift_y(w_down_two, -1)
    low_below = shift_y(w_down_two, 1)
    top_far = shift_y(top_above, -1)
    low_far = shift_y(low_above, -1)
    tops = (late_top, top_below, top_above, top_far)
    lows = (w_down_two, low_below, low_above, low_far)

    after_tiles = slab_exchange(after_own)
    parts = (early, below, twice, above)
    (w_held,) = local(
        load_parts,
        [((Y_COUNT - 1, LANES, width), half16)],
        *parts[:-1],
        scratch=(dma((Y_COUNT - 1,)),),
        outside=(0, 1, 2),
        held_out=True,
        vmem=True,
    )
    channels, residual = local(
        projections,
        [((Z_COUNT * 16, LANES), half16), ((slab_rows, LANES), half32)],
        after_tiles,
        mix_gain.reshape(1, -1),
        w_held,
        parts[-1],
        scratch=(
            pltpu.VMEM((slab_rows, width), half16),
            pltpu.VMEM((LANES, width), half16),
            dma((1,)),
        ),
        outside=(3,),
        held_out=True,
    )
    zgroups = [[a * Y_COUNT + b for a in range(Z_COUNT)] for b in range(Y_COUNT)]
    arrived = exchange(channels.reshape(Z_COUNT, 16, LANES), "kv", zgroups)
    held = state
    gated, vectors = local(
        read_state,
        [((seqs * heads, LANES), half32), ((seqs, 3 * heads, LANES), half32)],
        arrived.reshape(Z_COUNT * 16, LANES),
        forget_floor,
        floor_t,
        head_gain,
        held,
    )
    merged_tiles = slab_exchange(bf(gated))
    (new_state,) = local(
        next_state,
        [(state.shape, half32)],
        held,
        vectors,
        scratch=(pltpu.VMEM(state.shape, half32), dma((seqs,))),
        sent=(0,),
    )
    (w_mix,) = local(
        load_mix,
        [((Y_COUNT, own_cols, width), half16)],
        *parts,
        scratch=(dma((Y_COUNT,)),),
        outside=(0, 1, 2, 3),
        held_out=True,
        vmem=True,
    )
    (after_mix,) = local(
        mix_out,
        [((slab_rows, LANES), half16)],
        merged_tiles,
        w_mix,
        residual,
        scratch=(pltpu.VMEM((slab_rows, width), half16),),
    )

    mix_tiles = slab_exchange(after_mix)
    (w_held,) = local(
        load_parts,
        [((Y_COUNT - 1, 2 * hidden, width), half16)],
        *tops[:-1],
        scratch=(dma((Y_COUNT - 1,)),),
        outside=(0, 1, 2),
        vmem=True,
    )
    (messages,) = local(
        second_block,
        [((KV_COUNT * TP_COUNT, 8, LANES), half16)],
        mix_tiles,
        ffn_gain_two.reshape(1, -1),
        after_mix,
        w_held,
        tops[-1],
        *lows,
        scratch=(
            pltpu.VMEM((slab_rows, width), half16),
            pltpu.VMEM((2 * hidden, width), half16),
            pltpu.VMEM((Y_COUNT, hidden, width), half16),
            dma((Y_COUNT + 1,)),
        ),
        outside=(4, 5, 6, 7, 8),
    )
    arrived = exchange(messages, ("kv", "tp"))
    (result,) = local(finish, [((own_cols, rows), half16)], arrived)
    return (result.T, new_state)


def solution(mesh):
    return jax.shard_map(
        shards,
        mesh=mesh,
        in_specs=(
            P("dp", ("kv", "tp")),
            P(("dp", "kv"), "tp", None, None),
            P("tp", None),
            P(),
            P(None, ("kv", "tp")),
            P(None, ("kv", "tp")),
            P(("kv", "tp"), None),
            P(),
            P(None, "tp", "kv"),
            P(None, "tp", "kv"),
            P(None, "tp", "kv"),
            P(None, "tp", "kv"),
            P("tp", None),
            P(None, ("kv", "tp")),
            P(),
            P(None, ("kv", "tp")),
            P(None, ("kv", "tp")),
            P(("kv", "tp"), None),
        ),
        out_specs=(P("dp", ("kv", "tp")), P(("dp", "kv"), "tp", None, None)),
        check_vma=False,
    )
```
